512 devices in a mesh: sp: 64 (over z, y), tp: 8 (over x, core).
Axes of the slice: x: 4, y: 4, z: 16, core: 2. Of those that a mesh axis runs over, the one named last changes fastest.
Arguments:
- target: bfloat16 [8192, 2048], P('sp'), may hold values from -0.375 to 0.375
- source: bfloat16 [16384, 2048], P(('sp', 'tp')), may hold values from -0.375 to 0.375
- target_gain: float32 [2048], replicated, may hold values from 0.3 to 12
- source_gain: float32 [2048], replicated, may hold values from 0.3 to 12
- w_query: bfloat16 [2048, 1024], P(None, 'tp'), may hold values from -0.125 to 0.125
- w_key: bfloat16 [2048, 256], replicated, may hold values from -0.125 to 0.125
- w_value: bfloat16 [2048, 256], replicated, may hold values from -0.125 to 0.125
- attended: bfloat16 [8192, 1024], P('sp', 'tp'), may hold values from -6 to 6
- d_attended: bfloat16 [8192, 1024], P('sp', 'tp'), may hold values from -24 to 24
Outputs:
- d_target: bfloat16 [8192, 2048], P('sp')
- d_source: float32 [16384, 2048], P(('sp', 'tp'))
- d_w_query: float32 [2048, 1024], P('sp', 'tp')
The draws below stay inside these ranges and needn't reach their ends.
All inputs are finite; a program needn't handle non-finite values.
Results may differ from the reference program's by a relative error of at most 0.02.
The reference program's roundings to bfloat16 on the way count: a program that leaves them out, or rounds other values in their place, can miss the bound.
Values may be sent and summed in bfloat16 or wider, within the bound.
A program may use at most 64 MiB of HBM per device.

```python
import jax
import jax.numpy as jnp
from jax import lax

D = 2048
HQ = 8
KVH = 2
HD = 128
TT = 8192
SS = 16384


def gain_law(key):
    return jax.random.uniform(key, (D,), jnp.float32, 0.3, 1.7)


def draw_target_gain(key, part):
    return gain_law(jax.random.fold_in(key, 11))


def draw_source_gain(key, part):
    return gain_law(jax.random.fold_in(key, 23))


def level_of(rng, extent, pieces, least, largest):
    factor_of = 1.0
    for position, parts in pieces:
        heights = jax.random.uniform(jax.random.fold_in(jax.random.fold_in(rng, 6), position), (parts,), jnp.float32, least / len(pieces), largest / len(pieces))
        factor_of = factor_of * jnp.repeat(jnp.exp(heights), extent[position] // parts).reshape((-1,) + (1,) * (len(extent) - 1 - position))
    return factor_of


def gaussian(key, dims, deviation, most, shards=(), held_as=jnp.bfloat16):
    loudness = level_of(key, dims, shards, -0.22, 0.18) if shards else 1.0
    array = jax.random.normal(key, dims, jnp.float32) * deviation * loudness
    return jnp.minimum(jnp.maximum(array, -most), most).astype(held_as)


def setup_inputs(seed: int = 0) -> dict:
    key_of = jax.random.split(jax.random.key(seed), 10)
    target = gaussian(key_of[0], (TT, D), 0.0625, 0.375, ((0, 64),))
    source = gaussian(key_of[1], (SS, D), 0.0625, 0.375, ((0, 512),))
    target_gain = draw_target_gain(jax.random.fold_in(key_of[9], 71), 0)
    source_gain = draw_source_gain(jax.random.fold_in(key_of[9], 71), 0)
    w_query = gaussian(key_of[4], (D, HQ * HD), D ** -0.5, 0.125, ((1, 8),))
    w_key = gaussian(key_of[5], (D, KVH * HD), D ** -0.5, 0.125)
    w_value = gaussian(key_of[6], (D, KVH * HD), D ** -0.5, 0.125)
    attended = gaussian(key_of[7], (TT, HQ * HD), 1.0, 6.0, ((0, 64), (1, 8)))
    d_attended = gaussian(key_of[8], (TT, HQ * HD), 4.0, 24.0, ((0, 64), (1, 8)))
    return {"target": target, "source": source, "target_gain": target_gain, "source_gain": source_gain, "w_query": w_query, "w_key": w_key, "w_value": w_value, "attended": attended, "d_attended": d_attended}


EPS = 1e-06

def norm_rows(matrix, gain_vector):
    widened = matrix.astype(jnp.float32)
    inverse = lax.rsqrt(lax.optimization_barrier(jnp.mean(widened * widened, axis=-1, keepdims=True)) + EPS)
    return widened * inverse * gain_vector

def norm_back(matrix, gain_vector, cotangent):
    _, pullback = jax.vjp(lambda values: norm_rows(values, gain_vector), matrix.astype(jnp.float32))
    return pullback(cotangent)[0]

def block_count(row_count, most_rows):
    number = 1
    while row_count % (number * 2) == 0 and row_count // number > most_rows:
        number = number * 2
    return number

def reference(target, source, target_gain, source_gain, w_query, w_key, w_value, attended, d_attended):
    scaling = HD ** (-0.5)
    group_size = HQ // KVH
    normed_target = norm_rows(target, target_gain).astype(jnp.bfloat16)
    normed_source = norm_rows(source, source_gain).astype(jnp.bfloat16)
    query = jnp.dot(normed_target, w_query, preferred_element_type=jnp.float32).astype(jnp.bfloat16)
    key = jnp.dot(normed_source, w_key, preferred_element_type=jnp.float32).astype(jnp.bfloat16)
    value = jnp.dot(normed_source, w_value, preferred_element_type=jnp.float32).astype(jnp.bfloat16)
    target_total = query.shape[0]
    source_total = key.shape[0]
    delta = lax.optimization_barrier(jnp.sum(d_attended.astype(jnp.float32).reshape(target_total, HQ, HD) * attended.astype(jnp.float32).reshape(target_total, HQ, HD), axis=-1)).astype(jnp.bfloat16)
    number = block_count(target_total, 512)
    block_rows = target_total // number

    def one_head(head_index):
        kv_index = head_index // group_size
        query_head = lax.dynamic_slice_in_dim(query, head_index * HD, HD, 1)
        key_head = lax.dynamic_slice_in_dim(key, kv_index * HD, HD, 1)
        value_head = lax.dynamic_slice_in_dim(value, kv_index * HD, HD, 1)
        grad_head = lax.dynamic_slice_in_dim(d_attended, head_index * HD, HD, 1)
        delta_head = lax.dynamic_slice_in_dim(delta, head_index, 1, 1)[:, 0]
        query_blocks = query_head.reshape(number, block_rows, HD)
        grad_blocks = grad_head.reshape(number, block_rows, HD)
        delta_blocks = delta_head.reshape(number, block_rows)

        def totals_of(queries):
            scores = jnp.dot(queries, key_head.T, preferred_element_type=jnp.float32) * scaling
            maxima = lax.optimization_barrier(jnp.max(scores, axis=-1))
            return maxima + jnp.log(lax.optimization_barrier(jnp.sum(jnp.exp(scores - maxima[:, None]), axis=-1)))
        log_total = lax.map(totals_of, query_blocks)

        def grad_step(carried, blocks):
            queries, cotangent, totals, delta_rows = blocks
            scores = jnp.dot(queries, key_head.T, preferred_element_type=jnp.float32) * scaling
            weights = jnp.exp(scores - totals[:, None])
            d_weights = jnp.dot(cotangent, value_head.T, preferred_element_type=jnp.float32)
            d_scores = (weights * (d_weights - delta_rows.astype(jnp.float32)[:, None])).astype(jnp.bfloat16)
            query_grad = jnp.dot(d_scores, key_head, preferred_element_type=jnp.float32) * scaling
            key_acc = carried[0] + jnp.dot(d_scores.T, queries, preferred_element_type=jnp.float32) * scaling
            value_acc = carried[1] + jnp.dot(weights.astype(jnp.bfloat16).T, cotangent, preferred_element_type=jnp.float32)
            return ((key_acc, value_acc), query_grad)
        start_state = (jnp.zeros((source_total, HD), jnp.float32), jnp.zeros((source_total, HD), jnp.float32))
        (key_acc, value_acc), query_grads = lax.scan(grad_step, start_state, (query_blocks, grad_blocks, log_total, delta_blocks))
        return (key_acc, value_acc, query_grads.reshape(target_total, HD))
    key_grads, value_grads, query_grads = lax.map(one_head, jnp.arange(HQ, dtype=jnp.int32))
    d_key = key_grads.reshape(KVH, group_size, source_total, HD).sum(axis=1)
    d_value = value_grads.reshape(KVH, group_size, source_total, HD).sum(axis=1)
    d_key_b = d_key.transpose(1, 0, 2).reshape(source_total, KVH * HD).astype(jnp.bfloat16)
    d_value_b = d_value.transpose(1, 0, 2).reshape(source_total, KVH * HD).astype(jnp.bfloat16)
    d_query_b = query_grads.transpose(1, 0, 2).reshape(target_total, HQ * HD).astype(jnp.bfloat16)
    d_w_query = jnp.dot(normed_target.T, d_query_b, preferred_element_type=jnp.float32)
    d_normed_target = jnp.dot(d_query_b, w_query.T, preferred_element_type=jnp.float32)
    d_target = norm_back(target, target_gain, d_normed_target).astype(jnp.bfloat16)
    d_normed_source = jnp.dot(d_key_b, w_key.T, preferred_element_type=jnp.float32) + jnp.dot(d_value_b, w_value.T, preferred_element_type=jnp.float32)
    d_source = norm_back(source, source_gain, d_normed_source)
    return (d_target, d_source, d_w_query)
```

```python
import functools
import math

import jax
import jax.numpy as jnp
from jax import lax
from jax.experimental import pallas as pl
from jax.experimental.pallas import tpu as pltpu
from jax.sharding import Mesh
from jax.sharding import PartitionSpec as P

HD = 128
EPS = 1e-06
SCALE = HD ** (-0.5)
NZ, NY, NX, NC = 16, 4, 4, 2
PLANE = 16
MESH = pl.DeviceIdType.MESH
F32 = jnp.float32
BF16 = jnp.bfloat16
NT = (((1,), (1,)), ((), ()))


def norm_rows(matrix, gain_vector):
    widened = matrix.astype(F32)
    inverse = lax.rsqrt(jnp.mean(widened * widened, axis=-1, keepdims=True) + EPS)
    return widened * inverse * gain_vector


def norm_back(matrix, gain_vector, cotangent):
    _, pullback = jax.vjp(lambda values: norm_rows(values, gain_vector), matrix.astype(F32))
    return pullback(cotangent)[0]


def coords():
    return tuple(lax.axis_index(a) for a in ("z", "y", "x", "c"))


def plane_peers(me, with_self=False):
    z, y, x, c = me
    out = []
    for dy in (2, 1, 3, 0):
        for dx in (1, 0):
            for dc in (1, 0):
                if (dy, dx, dc) == (0, 0, 0) and not with_self:
                    continue
                y2 = lax.rem(y + dy, NY)
                xl2 = lax.rem(lax.rem(x, 2) + dx, 2)
                c2 = lax.rem(c + dc, 2)
                out.append(((z, y2, (x // 2) * 2 + xl2, c2), y2 * 4 + xl2 * 2 + c2))
    return out


def line_peers(me):
    z, y, x, c = me
    out = []
    for dz in (8, 7, 9, 6, 10, 5, 11, 4, 12, 3, 13, 2, 14, 1, 15, 0):
        for dh in (1, 0):
            if (dz, dh) == (0, 0):
                continue
            z2 = lax.rem(z + dz, NZ)
            h2 = lax.rem(x // 2 + dh, 2)
            out.append(((z2, y, h2 * 2 + lax.rem(x, 2), c), z2, h2))
    return out


def y_peers(me):
    z, y, x, c = me
    return [((z, lax.rem(y + dy, NY), x, c), lax.rem(y + dy, NY)) for dy in (2, 1, 3)]


def z_peers(me):
    z, y, x, c = me
    order = (8, 7, 9, 6, 10, 5, 11, 4, 12, 3, 13, 2, 14, 1, 15)
    return [((lax.rem(z + dz, NZ), y, x, c), lax.rem(z + dz, NZ)) for dz in order]


def tp_peers(me):
    z, y, x, c = me
    out = []
    for dx in (2, 1, 3, 0):
        for dc in (1, 0):
            if (dx, dc) == (0, 0):
                continue
            x2 = lax.rem(x + dx, NX)
            c2 = lax.rem(c + dc, 2)
            out.append(((z, y, x2, c2), x2 * 2 + c2))
    return out


def greet(devices):
    barrier = pltpu.get_barrier_semaphore()
    for d in devices:
        pl.semaphore_signal(barrier, inc=1, device_id=d, device_id_type=MESH)
    pl.semaphore_wait(barrier, len(devices))


def exchange(copies, send, recv):
    started = []
    for k, (src, dst, dev) in enumerate(copies):
        cp = pltpu.make_async_remote_copy(
            src_ref=src, dst_ref=dst, send_sem=send.at[k], recv_sem=recv.at[k],
            device_id=dev, device_id_type=MESH)
        cp.start()
        started.append(cp)
    return started


def comm_call(body, outs, count, cid, *args):
    vm = pl.BlockSpec(memory_space=pltpu.VMEM)
    return pl.pallas_call(
        body,
        out_shape=outs,
        in_specs=[vm] * len(args),
        out_specs=[vm] * len(outs),
        scratch_shapes=[pltpu.SemaphoreType.DMA((count,)), pltpu.SemaphoreType.DMA((count,))],
        compiler_params=pltpu.CompilerParams(collective_id=cid, has_side_effects=True),
        name="comm%d" % cid,
    )(*args)


def gather_body(q, do, dl, kv, q_all, do_all, dl_all, kv_all, send, recv):
    me = coords()
    z, y, x, c = me
    plane = plane_peers(me)
    line = line_peers(me)
    mine = y * 4 + lax.rem(x, 2) * 2 + c
    rows = pl.ds(pl.multiple_of(mine * 128, 128), 128)
    xh = x // 2
    kvrows = pl.ds(pl.multiple_of(z * 64 + xh * 32, 32), 32)
    greet([d for d, _ in plane] + [d for d, _, _ in line])
    copies = [(kv.at[h2], kv_all.at[kvrows, :], d) for d, _, h2 in line]
    copies += [(q, q_all.at[rows, :], d) for d, _ in plane]
    copies += [(do, do_all.at[rows, :], d) for d, _ in plane]
    copies += [(dl, dl_all.at[mine], d) for d, _ in plane]
    started = exchange(copies, send, recv)
    q_all[rows, :] = q[...]
    do_all[rows, :] = do[...]
    dl_all[mine] = dl[...]
    kv_all[kvrows, :] = kv[xh]
    for cp in started:
        cp.wait()


def stats_body(st, st_all, send, recv):
    me = coords()
    z, y, x, c = me
    plane = plane_peers(me)
    mine = y * 4 + lax.rem(x, 2) * 2 + c
    greet([d for d, _ in plane])
    started = exchange([(st, st_all.at[mine], d) for d, _ in plane], send, recv)
    st_all[mine] = st[...]
    for cp in started:
        cp.wait()


def scatter_body(dq, dkv, dq_in, dkv_in, send, recv):
    me = coords()
    z, y, x, c = me
    plane = plane_peers(me)
    line = line_peers(me)
    mine = y * 4 + lax.rem(x, 2) * 2 + c
    xh = x // 2
    greet([d for d, _ in plane] + [d for d, _, _ in line])
    copies = [(dkv.at[z2, h2], dkv_in.at[xh, z], d) for d, z2, h2 in line]
    copies += [(dq.at[j], dq_in.at[mine], d) for d, j in plane]
    started = exchange(copies, send, recv)
    dq_in[mine] = dq[mine]
    dkv_in[xh, z] = dkv[z, xh]
    for cp in started:
        cp.wait()


def tail1_body(dw, dn, dw_in, dn_in, send, recv):
    me = coords()
    z, y, x, c = me
    ys = y_peers(me)
    tps = tp_peers(me)
    tp = x * 2 + c
    greet([d for d, _ in ys] + [d for d, _ in tps])
    copies = [(dw.at[y2], dw_in.at[y], d) for d, y2 in ys]
    copies += [(dn.at[t2], dn_in.at[tp], d) for d, t2 in tps]
    started = exchange(copies, send, recv)
    dw_in[y] = dw[y]
    dn_in[tp] = dn[tp]
    for cp in started:
        cp.wait()


def tail2_body(dw, dt, dw_in, dt_in, send, recv):
    me = coords()
    z, y, x, c = me
    zs = z_peers(me)
    tps = tp_peers(me)
    tp = x * 2 + c
    greet([d for d, _ in zs] + [d for d, _ in tps])
    copies = [(dw.at[z2], dw_in.at[z], d) for d, z2 in zs]
    copies += [(dt, dt_in.at[tp], d) for d, t2 in tps]
    started = exchange(copies, send, recv)
    dw_in[z] = dw[z]
    dt_in[tp] = dt[...]
    for cp in started:
        cp.wait()


def stats_kernel(q_all, kv_all, st, s_scr):
    def pair(p, carry):
        q = q_all[pl.ds(pl.multiple_of(p * 256, 256), 256), :]
        top = None
        for k in range(4):
            s = lax.dot_general(kv_all[k * 256:(k + 1) * 256, :128], q, NT,
                                preferred_element_type=F32) * SCALE
            s_scr[k * 256:(k + 1) * 256, :] = s
            part = jnp.max(s.reshape(32, 8, 256), axis=0)
            top = part if top is None else jnp.maximum(top, part)
        m = jnp.max(top, axis=0, keepdims=True)
        tot = None
        for k in range(4):
            e = jnp.exp(s_scr[k * 256:(k + 1) * 256, :] - m)
            part = jnp.sum(e.reshape(32, 8, 256), axis=0)
            tot = part if tot is None else tot + part
        l = jnp.sum(tot, axis=0, keepdims=True)
        st[pl.ds(2 * p, 1), :] = m[:, :128]
        st[pl.ds(2 * p + 1, 1), :] = m[:, 128:]
        st[pl.ds(2 * p + 16, 1), :] = l[:, :128]
        st[pl.ds(2 * p + 17, 1), :] = l[:, 128:]
        return carry

    lax.fori_loop(0, 8, pair, 0)


def grads_kernel(q_all, do_all, dl_all, kv_all, st_all, dq, dkv, pt, ut, kt, lt):
    kt[...] = jnp.transpose(kv_all[:, :128])
    top = jnp.max(st_all[:, 0:16, :], axis=0)
    total = jnp.zeros((16, 128), F32)
    for j in range(16):
        total = total + st_all[j, 16:32, :] * jnp.exp(st_all[j, 0:16, :] - top)
    lt[...] = top + jnp.log(total)

    def pair(p, carry):
        rows = pl.ds(pl.multiple_of(p * 256, 256), 256)
        q = q_all[rows, :]
        do = do_all[rows, :]
        lrow = jnp.concatenate([lt[pl.ds(2 * p, 1), :], lt[pl.ds(2 * p + 1, 1), :]], axis=1)
        drow = jnp.concatenate([dl_all[2 * p, 0:1, :], dl_all[2 * p + 1, 0:1, :]], axis=1)
        for k in range(4):
            blk = slice(k * 256, (k + 1) * 256)
            s = lax.dot_general(kv_all[blk, :128], q, NT, preferred_element_type=F32) * SCALE
            w = jnp.exp(s - lrow)
            pt[blk, rows] = w.astype(BF16)
            g = lax.dot_general(kv_all[blk, 128:], do, NT, preferred_element_type=F32)
            ut[blk, rows] = (w * (g - drow)).astype(BF16)
        dqt = lax.dot_general(kt[...], ut[:, rows], (((1,), (0,)), ((), ())),
                              preferred_element_type=F32) * SCALE
        dq[rows, :] = jnp.transpose(dqt).astype(BF16)
        return carry

    lax.fori_loop(0, 8, pair, 0)

    def block(k, carry):
        rows = pl.ds(pl.multiple_of(k * 256, 256), 256)
        dk = jnp.dot(ut[rows, :], q_all[...], preferred_element_type=F32) * SCALE
        dv = jnp.dot(pt[rows, :], do_all[...], preferred_element_type=F32)
        dkv[rows, :] = jnp.concatenate([dk, dv], axis=1).astype(BF16)
        return carry

    lax.fori_loop(0, 4, block, 0)


def local_call(body, outs, scratch, name, flops, *args):
    vm = pl.BlockSpec(memory_space=pltpu.VMEM)
    return pl.pallas_call(
        body,
        out_shape=outs,
        in_specs=[vm] * len(args),
        out_specs=[vm] * len(outs),
        scratch_shapes=scratch,
        compiler_params=pltpu.CompilerParams(vmem_limit_bytes=48 * 1024 * 1024),
        cost_estimate=pl.CostEstimate(flops=flops, bytes_accessed=1 << 20, transcendentals=0),
        name=name,
    )(*args)


def shape(*dims, dtype=BF16):
    return jax.ShapeDtypeStruct(dims, dtype)


def local(target, source, target_gain, source_gain, w_query, w_key, w_value, attended, d_attended):
    z, y, x, c = coords()
    nt = norm_rows(target, target_gain).astype(BF16)
    ns = norm_rows(source, source_gain).astype(BF16)
    query = jnp.dot(nt, w_query, preferred_element_type=F32).astype(BF16)
    key = jnp.dot(ns, w_key, preferred_element_type=F32).astype(BF16)
    value = jnp.dot(ns, w_value, preferred_element_type=F32).astype(BF16)
    kv = jnp.stack([jnp.concatenate([key[:, :128], value[:, :128]], axis=1),
                    jnp.concatenate([key[:, 128:], value[:, 128:]], axis=1)])
    delta = jnp.sum(d_attended.astype(F32) * attended.astype(F32), axis=-1)
    delta = lax.reduce_precision(delta, 8, 7)
    dl = jnp.broadcast_to(delta[None, :], (8, 128))

    q_all, do_all, dl_all, kv_all = comm_call(
        gather_body,
        [shape(2048, 128), shape(2048, 128), shape(16, 8, 128, dtype=F32), shape(1024, 256)],
        31 + 45, 0, query, d_attended, dl, kv)
    st, = local_call(stats_kernel, [shape(32, 128, dtype=F32)],
                     [pltpu.VMEM((1024, 256), F32)], "stats", 1 << 30, q_all, kv_all)
    st_all, = comm_call(stats_body, [shape(16, 32, 128, dtype=F32)], 15, 1, st)
    dq, dkv = local_call(
        grads_kernel, [shape(2048, 128), shape(1024, 256)],
        [pltpu.VMEM((1024, 2048), BF16), pltpu.VMEM((1024, 2048), BF16),
         pltpu.VMEM((128, 1024), BF16), pltpu.VMEM((16, 128), F32)],
        "grads", 1 << 32, q_all, do_all, dl_all, kv_all, st_all)
    dq_in, dkv_in = comm_call(
        scatter_body, [shape(16, 128, 128), shape(2, 16, 32, 256)], 46, 2,
        dq.reshape(16, 128, 128), dkv.reshape(16, 2, 32, 256))
    dqb = jnp.sum(dq_in.astype(F32), axis=0).astype(BF16)
    dw = lax.dot_general(nt, dqb, (((0,), (0,)), ((), ())), preferred_element_type=F32)
    dw = dw.astype(BF16).reshape(16, 4, 32, 128).transpose(1, 0, 2, 3)
    dn = lax.dot_general(dqb, w_query, NT, preferred_element_type=F32).astype(BF16)
    dw_in, dn_in = comm_call(tail1_body, [shape(4, 16, 32, 128), shape(8, 16, 2048)], 10, 3,
                             dw, dn.reshape(8, 16, 2048))
    dw1 = jnp.sum(dw_in.astype(F32), axis=0).astype(BF16)
    dnt = jnp.sum(dn_in.astype(F32), axis=0)
    own = lax.dynamic_slice_in_dim(target, (x * 2 + c) * 16, 16, 0)
    dt = norm_back(own, target_gain, dnt).astype(BF16)
    dw2, d_target = comm_call(tail2_body, [shape(16, 32, 128), shape(8, 16, 2048)], 22, 4, dw1, dt)
    d_w_query = jnp.sum(dw2.astype(F32), axis=0)
    dkv_sum = jnp.sum(dkv_in.astype(F32), axis=1).astype(BF16)
    dkey = jnp.concatenate([dkv_sum[0, :, :128], dkv_sum[1, :, :128]], axis=1)
    dval = jnp.concatenate([dkv_sum[0, :, 128:], dkv_sum[1, :, 128:]], axis=1)
    dns = lax.dot_general(dkey, w_key, NT, preferred_element_type=F32) + lax.dot_general(
        dval, w_value, NT, preferred_element_type=F32)
    d_source = norm_back(source, source_gain, dns)
    return d_target.reshape(128, 2048), d_source, d_w_query


def solution(mesh):
    fine = Mesh(mesh.devices.reshape(NZ, NY, NX, NC), ("z", "y", "x", "c"))
    sp = ("z", "y")
    tp = ("x", "c")
    both = ("z", "y", "x", "c")
    placed = (P(sp, None), P(both, None), P(), P(), P(None, tp), P(), P(), P(sp, tp), P(sp, tp))
    return jax.shard_map(
        local, mesh=fine, in_specs=placed,
        out_specs=(P(sp, None), P(both, None), P(sp, tp)), check_vma=False)
```

```python
import jax
import jax.numpy as jnp
from jax import lax
from jax.experimental import pallas as pl
from jax.experimental.pallas import tpu as pltpu
from jax.sharding import Mesh
from jax.sharding import PartitionSpec as P

HD = 128
EPS = 1e-06
SCALE = HD ** (-0.5)
NZ, NY, NX, NC = 16, 4, 4, 2
MESH = pl.DeviceIdType.MESH
F32 = jnp.float32
BF16 = jnp.bfloat16
NT = (((1,), (1,)), ((), ()))
NN = (((1,), (0,)), ((), ()))
MESSAGES = 128


def dot(a, b, dims=NN):
    return lax.dot_general(a, b, dims, preferred_element_type=F32)


def normed(matrix, gain):
    wide = matrix.astype(F32)
    inverse = lax.rsqrt(jnp.mean(wide * wide, axis=-1, keepdims=True) + EPS)
    return (wide * inverse * gain).astype(BF16)


def normed_back(matrix, gain, cotangent):
    wide = matrix.astype(F32)
    inverse = lax.rsqrt(jnp.mean(wide * wide, axis=-1, keepdims=True) + EPS)
    scaled = cotangent * gain
    along = jnp.mean(scaled * wide, axis=-1, keepdims=True)
    return scaled * inverse - wide * (inverse * inverse * inverse * along)


def kernel(target, source, tgain, sgain, w_query, w_key, w_value, attended, d_attended,
           d_target, d_source, d_w,
           tg, sr, wq, wk, wv, nt_t, kv_own, kv, qd, st, st_all, lt, mg, lg,
           s_scr, g_scr, pt, ut, kt, dq, dq_in, dkv, near1, near2, near3, near4,
           far, far_in, dw, dw_in, dw1, dw2, dn, dn_in, load_sem, send_sem, recv_sem):
    z = lax.axis_index("z")
    y = lax.axis_index("y")
    x = lax.axis_index("x")
    c = lax.axis_index("c")
    xh = x // 2
    xl = lax.rem(x, 2)
    mine = y * 4 + xl * 2 + c
    tp = x * 2 + c

    def zmod(v):
        return lax.rem(v + NZ, NZ)

    def at(dz=0, dy=0, dxl=0, dc=0, dh=0):
        x2 = lax.rem(xh + dh, 2) * 2 + lax.rem(xl + dxl, 2)
        return (zmod(z + dz), lax.rem(y + dy, NY), x2, lax.rem(c + dc, 2))

    def block(dy, dxl, dc):
        return lax.rem(y + dy + NY, NY) * 4 + lax.rem(xl + dxl, 2) * 2 + lax.rem(c + dc, 2)

    def rows_of(j, n=128):
        return pl.ds(pl.multiple_of(j * n, n), n)

    count = [0]
    pending = []

    def remote(src, dst, dev):
        k = count[0]
        count[0] += 1
        cp = pltpu.make_async_remote_copy(
            src_ref=src, dst_ref=dst, send_sem=send_sem.at[k], recv_sem=recv_sem.at[k],
            device_id=dev, device_id_type=MESH)
        cp.start()
        pending.append(cp)
        return cp

    loads = []
    for k, (a, b) in enumerate(((source, sr), (w_key, wk), (w_value, wv), (target, tg), (w_query, wq))):
        cp = pltpu.make_async_copy(a, b, load_sem.at[k])
        cp.start()
        loads.append(cp)

    offs = [(dy, dx, dc) for dy in (2, 1, 3, 0) for dx in (1, 0) for dc in (1, 0)][:-1]
    tps = [(dh, dx, dc) for dh in (1, 0) for dx in (1, 0) for dc in (1, 0)][:-1]
    peers = [at(dy=a, dxl=b, dc=d) for a, b, d in offs]
    peers += [at(dz=k) for k in range(1, 16)]
    peers += [at(dz=k, dh=1) for k in (4, 8, 12)]
    peers += [at(dh=1, dxl=a, dc=b) for a in (0, 1) for b in (0, 1)]
    barrier = pltpu.get_barrier_semaphore()
    for d in peers:
        pl.semaphore_signal(barrier, inc=1, device_id=d, device_id_type=MESH)

    loads[0].wait()
    ns = normed(sr[...], sgain[...])
    loads[1].wait()
    loads[2].wait()
    key = dot(ns, wk[...]).astype(BF16)
    value = dot(ns, wv[...]).astype(BF16)
    kv_own[0] = jnp.concatenate([key[:, :128], value[:, :128]], axis=1)
    kv_own[1] = jnp.concatenate([key[:, 128:], value[:, 128:]], axis=1)
    pl.semaphore_wait(barrier, len(peers))

    g1 = {}
    for k, dh in ((0, 1), (2, 0), (2, 1), (1, 0), (1, 1), (3, 0), (3, 1)):
        slot = (4 - k) % 4
        g1[slot, dh] = remote(kv_own.at[lax.rem(xh + dh, 2)],
                              kv.at[pl.ds(slot * 64 + dh * 32, 32), :], at(dz=4 * k, dh=dh))
    kv[0:32, :] = kv_own[xh]

    loads[3].wait()
    nt = normed(tg[...], tgain[...])
    loads[4].wait()
    query = dot(nt, wq[...]).astype(BF16)
    qd[0, rows_of(mine), :] = query
    qd[1, rows_of(mine), :] = d_attended[...]
    own_qd = qd.at[:, rows_of(mine), :]
    qsend = {}
    for dy, dx in ((2, 0), (2, 1), (1, 0), (3, 0), (1, 1), (3, 1), (0, 1)):
        qsend[dy, dx] = remote(own_qd, own_qd, at(dy=dy, dxl=dx))
    qpart = remote(own_qd, own_qd, at(dc=1))

    prod = d_attended[...].astype(F32) * attended[...].astype(F32)
    delta = jnp.sum(jnp.transpose(prod), axis=0, keepdims=True).astype(BF16).astype(F32)
    st[32:40, :] = jnp.broadcast_to(delta, (8, 128))
    nt_t[...] = jnp.transpose(nt)

    near = {}

    def chunk(g, k):
        return kv.at[pl.ds(g * 256 + k * 64, 64), :]

    def forward(k, steps):
        for d in steps:
            if d == -1:
                dst = chunk(1, k)
            elif d == 1:
                dst = chunk(2, k)
            elif d == -2:
                dst = chunk(3, k)
            else:
                dst = chunk(3, {0: 3, 3: 2}[k])
            near[k, d] = remote(chunk(0, k), dst, at(dz=d))

    g1[0, 1].wait_recv()
    forward(0, (1, -1, 2, -2))
    qfwd = []
    for (dy, dx), cp in list(qsend.items())[2:]:
        cp.wait_recv()
        r = qd.at[:, rows_of(block(-dy, dx, 0)), :]
        qfwd.append(remote(r, r, at(dc=1)))
    for k, steps in ((1, (-2, 1, -1)), (3, (2, 1, -1))):
        g1[k, 0].wait_recv()
        g1[k, 1].wait_recv()
        forward(k, steps)
    for (dy, dx), cp in list(qsend.items())[:2]:
        cp.wait_recv()
        r = qd.at[:, rows_of(block(-dy, dx, 0)), :]
        qfwd.append(remote(r, r, at(dc=1)))
    g1[2, 0].wait_recv()
    g1[2, 1].wait_recv()
    forward(2, (1, -1))
    qpart.wait_recv()
    for cp in qfwd:
        cp.wait_recv()

    def scores(g):
        def pair(p, carry):
            rows = rows_of(p, 256)
            blk = slice(g * 256, (g + 1) * 256)
            s = dot(kv[blk, :128], qd[0, rows, :], NT) * SCALE
            s_scr[blk, rows] = s
            m = jnp.max(s, axis=0, keepdims=True)
            mg[g:g + 1, rows] = m
            lg[g:g + 1, rows] = jnp.sum(jnp.exp(s - m), axis=0, keepdims=True)
            return carry
        lax.fori_loop(0, 8, pair, 0)

    def weights_back(g):
        def pair(p, carry):
            rows = rows_of(p, 256)
            blk = slice(g * 256, (g + 1) * 256)
            g_scr[blk, rows] = dot(kv[blk, 128:], qd[1, rows, :], NT)
            return carry
        lax.fori_loop(0, 8, pair, 0)
        kt[:, g * 256:(g + 1) * 256] = jnp.transpose(kv[g * 256:(g + 1) * 256, :128])

    scores(0)
    weights_back(0)
    for k in range(4):
        near[k, -1].wait_recv()
    scores(1)
    weights_back(1)
    for k in range(4):
        near[k, 1].wait_recv()
    scores(2)
    weights_back(2)
    for k, d in ((0, -2), (1, -2), (3, 2), (0, 2)):
        near[k, d].wait_recv()
    scores(3)

    m4 = mg[0:4, :]
    m1 = jnp.max(m4, axis=0, keepdims=True)
    l1 = jnp.sum(lg[0:4, :] * jnp.exp(m4 - m1), axis=0, keepdims=True)
    for j in range(16):
        st[j:j + 1, :] = m1[:, j * 128:(j + 1) * 128]
        st[j + 16:j + 17, :] = l1[:, j * 128:(j + 1) * 128]
    stats = [remote(st, st_all.at[mine], at(dy=a, dxl=b, dc=d)) for a, b, d in offs]
    st_all[mine] = st[...]
    weights_back(3)
    for cp in stats:
        cp.wait_recv()

    top = jnp.max(st_all[:, 0:16, :], axis=0)
    total = jnp.zeros((16, 128), F32)
    for j in range(16):
        total = total + st_all[j, 16:32, :] * jnp.exp(st_all[j, 0:16, :] - top)
    lt[...] = top + jnp.log(total)

    def grads(p, carry):
        rows = rows_of(p, 256)
        lrow = jnp.concatenate([lt[pl.ds(2 * p, 1), :], lt[pl.ds(2 * p + 1, 1), :]], axis=1)
        drow = jnp.concatenate([st_all[2 * p, 32:33, :], st_all[2 * p + 1, 32:33, :]], axis=1)
        for g in range(4):
            blk = slice(g * 256, (g + 1) * 256)
            w = jnp.exp(s_scr[blk, rows] - lrow)
            pt[blk, rows] = w.astype(BF16)
            ut[blk, rows] = (w * (g_scr[blk, rows] - drow)).astype(BF16)
        dqt = dot(kt[...], ut[:, rows]) * SCALE
        dq[rows, :] = jnp.transpose(dqt).astype(BF16)
        return carry

    lax.fori_loop(0, 8, grads, 0)
    dq_send = [remote(dq.at[rows_of(block(a, b, d)), :], dq_in.at[mine], at(dy=a, dxl=b, dc=d))
               for a, b, d in offs]
    dq_in[mine] = dq[rows_of(mine), :]

    def key_grads(g):
        blk = slice(g * 256, (g + 1) * 256)
        dk = dot(ut[blk, :], qd[0]) * SCALE
        dv = dot(pt[blk, :], qd[1])
        dkv[blk, :] = jnp.concatenate([dk, dv], axis=1).astype(BF16)

    key_grads(3)
    n3 = remote(dkv.at[pl.ds(768, 128), :], near3, at(dz=2))
    n4 = remote(dkv.at[pl.ds(896, 128), :], near4, at(dz=-2))
    key_grads(1)
    n1 = remote(dkv.at[pl.ds(256, 256), :], near1, at(dz=1))
    key_grads(2)
    n2 = remote(dkv.at[pl.ds(512, 256), :], near2, at(dz=-1))
    key_grads(0)

    for cp in dq_send:
        cp.wait_recv()
    acc = dq_in[0].astype(F32)
    for j in range(1, 16):
        acc = acc + dq_in[j].astype(F32)
    dqb = acc.astype(BF16)
    dw[...] = dot(nt_t[...], dqb).astype(BF16).reshape(16, 4, 32, 128)
    w_send = [remote(dw.at[:, lax.rem(y + d, NY)], dw_in.at[y], at(dy=d)) for d in (2, 1, 3)]
    dn[...] = dot(dqb, wq[...], NT).astype(BF16)
    n_send = []
    for a, b, d in tps:
        dev = at(dh=a, dxl=b, dc=d)
        n_send.append(remote(dn.at[rows_of(dev[2] * 2 + dev[3], 16), :], dn_in.at[tp], dev))
    dw_in[y] = dw[:, y]
    dn_in[tp] = dn[rows_of(tp, 16), :]

    for cp in (n3, n4, n1, n2):
        cp.wait_recv()
    base = near1[...].astype(F32) + near2[...].astype(F32) + dkv[0:256, :].astype(F32)
    x3 = near3[...].astype(F32)
    x4 = near4[...].astype(F32)
    far[0:64, :] = (base[0:64] + x3[0:64] + x4[64:128]).astype(BF16)
    far[64:128, :] = (base[64:128] + x3[64:128]).astype(BF16)
    far[128:192, :] = base[128:192].astype(BF16)
    far[192:256, :] = (base[192:256] + x4[0:64]).astype(BF16)
    f_send = []
    for k, dh in ((2, 0), (2, 1), (1, 0), (1, 1), (3, 0), (3, 1), (0, 1)):
        f_send.append(remote(far.at[pl.ds(k * 64 + dh * 32, 32), :], far_in.at[dh, k],
                             at(dz=4 * k, dh=dh)))
    far_in[0, 0] = far[0:32, :]

    for cp in w_send:
        cp.wait_recv()
    wsum = dw_in[0].astype(F32)
    for j in range(1, 4):
        wsum = wsum + dw_in[j].astype(F32)
    dw1[...] = wsum.astype(BF16)
    z_send = [remote(dw1.at[zmod(z + d)], dw2.at[z], at(dz=d))
              for d in (8, 7, 9, 6, 10, 5, 11, 4, 12, 3, 13, 2, 14, 1, 15)]
    dw2[z] = dw1[z]

    for cp in n_send:
        cp.wait_recv()
    nsum = dn_in[0].astype(F32)
    for j in range(1, 8):
        nsum = nsum + dn_in[j].astype(F32)
    d_target[rows_of(tp, 16), :] = normed_back(tg[rows_of(tp, 16), :], tgain[...], nsum).astype(BF16)
    own_t = d_target.at[rows_of(tp, 16), :]
    t_send = [remote(own_t, own_t, at(dh=a, dxl=b, dc=d)) for a, b, d in tps]

    for cp in f_send:
        cp.wait_recv()
    fs = []
    for dh in range(2):
        v = far_in[dh, 0].astype(F32)
        for k in range(1, 4):
            v = v + far_in[dh, k].astype(F32)
        fs.append(v)
    low = jnp.where(xh == 0, fs[0], fs[1]).astype(BF16)
    high = jnp.where(xh == 0, fs[1], fs[0]).astype(BF16)
    dkey = jnp.concatenate([low[:, :128], high[:, :128]], axis=1)
    dval = jnp.concatenate([low[:, 128:], high[:, 128:]], axis=1)
    dns = dot(dkey, wk[...], NT) + dot(dval, wv[...], NT)
    d_source[...] = normed_back(sr[...], sgain[...], dns)

    for cp in z_send:
        cp.wait_recv()
    zsum = dw2[0].astype(F32)
    for j in range(1, 16):
        zsum = zsum + dw2[j].astype(F32)
    d_w[...] = zsum
    for cp in t_send:
        cp.wait_recv()
    for cp in pending:
        cp.wait_send()


def local(target, source, target_gain, source_gain, w_query, w_key, w_value, attended, d_attended):
    vm = pl.BlockSpec(memory_space=pltpu.VMEM)
    anywhere = pl.BlockSpec(memory_space=pl.ANY)
    v = pltpu.VMEM
    return pl.pallas_call(
        kernel,
        out_shape=[jax.ShapeDtypeStruct((128, 2048), BF16), jax.ShapeDtypeStruct((32, 2048), F32),
                   jax.ShapeDtypeStruct((32, 128), F32)],
        in_specs=[anywhere, anywhere, vm, vm, anywhere, anywhere, anywhere, vm, vm],
        out_specs=[vm, vm, vm],
        scratch_shapes=[
            v((128, 2048), BF16), v((32, 2048), BF16), v((2048, 128), BF16),
            v((2048, 256), BF16), v((2048, 256), BF16), v((2048, 128), BF16),
            v((2, 32, 256), BF16), v((1024, 256), BF16), v((2, 2048, 128), BF16),
            v((40, 128), F32), v((16, 40, 128), F32), v((16, 128), F32),
            v((8, 2048), F32), v((8, 2048), F32),
            v((1024, 2048), F32), v((1024, 2048), F32),
            v((1024, 2048), BF16), v((1024, 2048), BF16), v((128, 1024), BF16),
            v((2048, 128), BF16), v((16, 128, 128), BF16), v((1024, 256), BF16),
            v((256, 256), BF16), v((256, 256), BF16), v((128, 256), BF16), v((128, 256), BF16),
            v((256, 256), BF16), v((2, 4, 32, 256), BF16),
            v((16, 4, 32, 128), BF16), v((4, 16, 32, 128), BF16), v((16, 32, 128), BF16),
            v((16, 32, 128), BF16), v((128, 2048), BF16), v((8, 16, 2048), BF16),
            pltpu.SemaphoreType.DMA((5,)), pltpu.SemaphoreType.DMA((MESSAGES,)),
            pltpu.SemaphoreType.DMA((MESSAGES,)),
        ],
        compiler_params=pltpu.CompilerParams(
            collective_id=0, has_side_effects=True, vmem_limit_bytes=56 * 1024 * 1024),
        name="step",
    )(target, source, target_gain.reshape(1, 2048), source_gain.reshape(1, 2048),
      w_query, w_key, w_value, attended, d_attended)


def solution(mesh):
    fine = Mesh(mesh.devices.reshape(NZ, NY, NX, NC), ("z", "y", "x", "c"))
    sp = ("z", "y")
    tp = ("x", "c")
    both = ("z", "y", "x", "c")
    placed = (P(sp, None), P(both, None), P(), P(), P(None, tp), P(), P(), P(sp, tp), P(sp, tp))
    return jax.shard_map(
        local, mesh=fine, in_specs=placed,
        out_specs=(P(sp, None), P(both, None), P(sp, tp)), check_vma=False)
```

```python
import jax
import jax.numpy as jnp
from jax import lax
from jax.experimental import pallas as pl
from jax.experimental.pallas import tpu as pltpu
from jax.sharding import Mesh
from jax.sharding import PartitionSpec as P

HD = 128
EPS = 1e-06
SCALE = HD ** (-0.5)
LOG2E = 1.4426950408889634
NZ, NY, NX, NC = 16, 4, 4, 2
MESH = pl.DeviceIdType.MESH
F32 = jnp.float32
BF16 = jnp.bfloat16
NT = (((1,), (1,)), ((), ()))
NN = (((1,), (0,)), ((), ()))
MESSAGES = 208
BASE = {0: 0, 1: 320, 3: 576, 2: 832}
SIZE = {0: 320, 1: 256, 3: 256, 2: 192}
NEAR = {0: (1, -1, 2, -2), 1: (-2, 1, -1), 3: (2, 1, -1), 2: (1, -1)}
ZORDER = (8, 7, 9, 6, 10, 5, 11, 4, 12, 3, 13, 2, 14, 1, 15, 0)


def dot(a, b, dims=NN):
    return lax.dot_general(a, b, dims, preferred_element_type=F32)


def place(k, d):
    if d == 0:
        slot = 0
    elif d == -1:
        slot = 1
    elif d == 1:
        slot = 2
    elif d == -2:
        slot = 3
    else:
        slot = 4 if k == 0 else 3
    return BASE[k] + 64 * slot


def normed(matrix, gain):
    wide = matrix.astype(F32)
    inverse = lax.rsqrt(jnp.mean(wide * wide, axis=-1, keepdims=True) + EPS)
    return (wide * inverse * gain).astype(BF16)


def normed_back(matrix, gain, cotangent):
    wide = matrix.astype(F32)
    inverse = lax.rsqrt(jnp.mean(wide * wide, axis=-1, keepdims=True) + EPS)
    scaled = cotangent * gain
    along = jnp.mean(scaled * wide, axis=-1, keepdims=True)
    return scaled * inverse - wide * (inverse * inverse * inverse * along)


def kernel(target, source, tgain, sgain, w_query, w_key, w_value, attended, d_attended,
           d_target, d_source, d_w,
           tg, sr, wq, wk, wv, tgn, sgn, att, dat, nt_t, kv_own, kv, q, do, dl, own_dl,
           st, st_all, mg, lg, e_scr, u_scr, pt, ut, kt, dqf, dq, dq_in, q_t, do_t, q2, do2, dkv, near_in,
           far, far_in, dw, dw_in, dw1, dw2, dn, dn_pair, dn2, dn_in,
           load_sem, send_sem, recv_sem):
    z = lax.axis_index("z")
    y = lax.axis_index("y")
    x = lax.axis_index("x")
    c = lax.axis_index("c")
    xh = x // 2
    xl = lax.rem(x, 2)
    mine = y * 4 + xl * 2 + c
    tp = x * 2 + c

    def zmod(v):
        return lax.rem(v + NZ, NZ)

    def at(dz=0, dy=0, dxl=0, dc=0, dh=0):
        x2 = lax.rem(xh + dh, 2) * 2 + lax.rem(xl + dxl, 2)
        return (zmod(z + dz), lax.rem(y + dy, NY), x2, lax.rem(c + dc, 2))

    def block(dy, dxl, dc):
        return lax.rem(y + dy + NY, NY) * 4 + lax.rem(xl + dxl, 2) * 2 + lax.rem(c + dc, 2)

    def rows_of(j, n=128):
        return pl.ds(pl.multiple_of(j * n, n), n)

    count = [0]
    pending = []

    def remote(src, dst, dev):
        k = count[0]
        count[0] += 1
        cp = pltpu.make_async_remote_copy(
            src_ref=src, dst_ref=dst, send_sem=send_sem.at[k], recv_sem=recv_sem.at[k],
            device_id=dev, device_id_type=MESH)
        cp.start()
        pending.append(cp)
        return cp

    loads = []
    for k, (a, b) in enumerate(((source, sr), (sgain, sgn), (w_key, wk), (w_value, wv),
                                (target, tg), (tgain, tgn), (w_query, wq),
                                (d_attended, dat), (attended, att))):
        cp = pltpu.make_async_copy(a, b, load_sem.at[k])
        cp.start()
        loads.append(cp)

    offs = [(dy, dx, dc) for dy in (2, 1, 3, 0) for dx in (1, 0) for dc in (1, 0)][:-1]
    peers = [at(dy=a, dxl=b, dc=d) for a, b, d in offs]
    peers += [at(dz=k) for k in range(1, 16)]
    peers += [at(dz=k, dh=1) for k in (4, 8, 12)]
    peers += [at(dh=1, dxl=a, dc=b) for a in (0, 1) for b in (0, 1)]
    barrier = pltpu.get_barrier_semaphore()
    for d in peers:
        pl.semaphore_signal(barrier, inc=1, device_id=d, device_id_type=MESH)

    for k in range(4):
        loads[k].wait()
    ns = normed(sr[...], sgn[...])
    key = dot(ns, wk[...]).astype(BF16)
    value = dot(ns, wv[...]).astype(BF16)
    kv_own[0] = jnp.concatenate([key[:, :128], value[:, :128]], axis=1)
    kv_own[1] = jnp.concatenate([key[:, 128:], value[:, 128:]], axis=1)
    pl.semaphore_wait(barrier, len(peers))

    g1 = {}
    for k, dh in ((0, 1), (2, 0), (2, 1), (1, 0), (1, 1), (3, 0), (3, 1)):
        slot = (4 - k) % 4
        g1[slot, dh] = remote(kv_own.at[lax.rem(xh + dh, 2)],
                              kv.at[pl.ds(place(slot, 0) + dh * 32, 32), :], at(dz=4 * k, dh=dh))
    kv[0:32, :] = kv_own[xh]

    for k in range(4, 9):
        loads[k].wait()
    nt = normed(tg[...], tgn[...])
    q[rows_of(mine), :] = dot(nt, wq[...]).astype(BF16)
    do[rows_of(mine), :] = dat[...]
    chips = ((2, 0), (2, 1), (1, 0), (3, 0), (1, 1), (3, 1), (0, 1))
    own_q = q.at[rows_of(mine), :]
    own_do = do.at[rows_of(mine), :]
    q_send = {o: remote(own_q, own_q, at(dy=o[0], dxl=o[1])) for o in chips}
    q_pair = remote(own_q, own_q, at(dc=1))
    prod = dat[...].astype(F32) * att[...].astype(F32)
    delta = jnp.sum(jnp.transpose(prod), axis=0, keepdims=True).astype(BF16).astype(F32)
    own_dl[...] = jnp.broadcast_to(delta, (8, 128))
    dl[mine] = own_dl[...]
    do_send = {o: remote(own_do, own_do, at(dy=o[0], dxl=o[1])) for o in chips}
    do_pair = remote(own_do, own_do, at(dc=1))
    dl_send = [remote(own_dl, dl.at[mine], at(dy=a, dxl=b, dc=d)) for a, b, d in offs]
    nt_t[...] = jnp.transpose(nt)

    near = {}

    def forward(k):
        src = kv.at[pl.ds(place(k, 0), 64), :]
        for d in NEAR[k]:
            near[k, d] = remote(src, kv.at[pl.ds(place(k, d), 64), :], at(dz=d))

    def pass_on(sends, array):
        out = []
        for dy, dx in ((0, 1), (1, 0), (3, 0), (1, 1), (3, 1), (2, 0), (2, 1)):
            sends[dy, dx].wait_recv()
            r = array.at[rows_of(block(-dy, dx, 0)), :]
            out.append(remote(r, r, at(dc=1)))
        return out

    def arrived(k):
        for d in NEAR[k]:
            near[k, d].wait_recv()

    def far_arrived(k):
        for dh in (0, 1):
            if (k, dh) != (0, 0):
                g1[k, dh].wait_recv()

    def scores(k):
        base, size = BASE[k], SIZE[k]

        def pair(p, carry):
            cols = rows_of(p, 256)
            s = dot(kv[base:base + size, :128], q_t[:, cols])
            for i in range(size // 64):
                t = s[i * 64:(i + 1) * 64].reshape(8, 8, 256) * (SCALE * LOG2E)
                m = jnp.max(t, axis=0)
                e = jnp.exp2(t - m[None])
                n = base // 64 + i
                mg[n, :, cols] = m
                lg[n, :, cols] = jnp.sum(e, axis=0)
                e_scr[base + i * 64:base + (i + 1) * 64, cols] = e.reshape(64, 256)
            return carry

        lax.fori_loop(0, 8, pair, 0, unroll=2)

    def weights_back(k):
        base, size = BASE[k], SIZE[k]

        def pair(p, carry):
            cols = rows_of(p, 256)
            g = dot(kv[base:base + size, 128:], do_t[:, cols])
            drow = jnp.concatenate([dl[2 * p, 0:1, :], dl[2 * p + 1, 0:1, :]], axis=1)
            u_scr[base:base + size, cols] = e_scr[base:base + size, cols] * (g - drow)
            return carry

        lax.fori_loop(0, 8, pair, 0, unroll=2)

    far_arrived(0)
    forward(0)
    q_fwd = pass_on(q_send, q)
    for k in (1, 3):
        far_arrived(k)
        forward(k)
    q_pair.wait_recv()
    for cp in q_fwd:
        cp.wait_recv()
    q_t[...] = jnp.transpose(q[...])
    arrived(0)
    scores(0)
    do_fwd = pass_on(do_send, do)
    arrived(1)
    scores(1)
    arrived(3)
    scores(3)
    far_arrived(2)
    forward(2)
    do_pair.wait_recv()
    for cp in do_fwd + dl_send:
        cp.wait_recv()
    do_t[...] = jnp.transpose(do[...])
    weights_back(0)
    kt[:, :832] = jnp.transpose(kv[:832, :128])
    arrived(2)
    scores(2)
    top8 = jnp.max(mg[...], axis=0)
    top1 = jnp.max(top8, axis=0, keepdims=True)
    tot = lg[0] * jnp.exp2(mg[0] - top1)
    for i in range(1, 16):
        tot = tot + lg[i] * jnp.exp2(mg[i] - top1)
    lse = top1 + jnp.log(jnp.sum(tot, axis=0, keepdims=True)) * LOG2E
    for j in range(16):
        st[j:j + 1, :] = lse[:, j * 128:(j + 1) * 128]
    stats = [remote(st, st_all.at[mine], at(dy=a, dxl=b, dc=d)) for a, b, d in offs]
    st_all[mine] = st[...]
    for i in range(16):
        mg[i] = jnp.exp2(mg[i] - lse)
    weights_back(1)
    weights_back(3)
    weights_back(2)
    kt[:, 832:] = jnp.transpose(kv[832:, :128])

    def grads(p, carry):
        cols = rows_of(p, 256)
        for i in range(16):
            r = slice(i * 64, (i + 1) * 64)
            f = mg[i, :, cols][None]
            pt[r, cols] = (e_scr[r, cols].reshape(8, 8, 256) * f).reshape(64, 256).astype(BF16)
            ut[r, cols] = (u_scr[r, cols].reshape(8, 8, 256) * f).reshape(64, 256).astype(BF16)
        dqf[cols, :] = jnp.transpose(dot(kt[...], ut[:, cols]) * SCALE)
        return carry

    lax.fori_loop(0, 8, grads, 0)
    for cp in stats:
        cp.wait_recv()
    top = jnp.max(st_all[...], axis=0)
    total = jnp.zeros((16, 128), F32)
    for j in range(16):
        total = total + jnp.exp2(st_all[j] - top)
    factor = jnp.exp2(st[...] - (top + jnp.log(total) * LOG2E))
    factor_t = jnp.transpose(jnp.concatenate([factor, jnp.zeros((112, 128), F32)], axis=0))
    for j in range(16):
        r = slice(j * 128, (j + 1) * 128)
        dq[r, :] = (dqf[r, :] * factor_t[:, j:j + 1]).astype(BF16)
    dq_send = [remote(dq.at[rows_of(block(a, b, d)), :], dq_in.at[mine], at(dy=a, dxl=b, dc=d))
               for a, b, d in offs]
    dq_in[mine] = dq[rows_of(mine), :]
    for j in range(16):
        r = slice(j * 128, (j + 1) * 128)
        f = factor_t[:, j:j + 1]
        q2[r, :] = (q[r, :].astype(F32) * f).astype(BF16)
        do2[r, :] = (do[r, :].astype(F32) * f).astype(BF16)
    back = {}
    index = 0
    for k in (2, 1, 3, 0):
        r = slice(BASE[k], BASE[k] + SIZE[k])
        dk = dot(ut[r, :], q2[...]) * SCALE
        dv = dot(pt[r, :], do2[...])
        dkv[r, :] = jnp.concatenate([dk, dv], axis=1).astype(BF16)
        for d in NEAR[k]:
            back[k, d] = (remote(dkv.at[pl.ds(place(k, d), 64), :], near_in.at[index], at(dz=-d)),
                          index)
            index += 1

    for cp in dq_send:
        cp.wait_recv()
    acc = dq_in[0].astype(F32)
    for j in range(1, 16):
        acc = acc + dq_in[j].astype(F32)
    dqb = acc.astype(BF16)
    w_all = dot(nt_t[...], dqb).astype(BF16)
    dn_all = dot(dqb, wq[...], NT).astype(BF16)
    dw[...] = w_all.reshape(16, 4, 32, 128)
    w_send = ([], [])
    for part in range(2):
        for d in (2, 1, 3):
            for i in range(8 * part, 8 * part + 8):
                w_send[part].append(remote(dw.at[zmod(z + ZORDER[i]), lax.rem(y + d, NY)],
                                           dw_in.at[i, y], at(dy=d)))
        if part == 0:
            dn[...] = dn_all.reshape(4, 2, 16, 2048)
            pair_send = remote(dn.at[:, lax.rem(c + 1, 2)], dn_pair, at(dc=1))
    for i in range(16):
        dw_in[i, y] = dw[zmod(z + ZORDER[i]), y]

    pair_send.wait_recv()
    dn2[...] = (dn[:, c].astype(F32) + dn_pair[...].astype(F32)).astype(BF16)
    n_send = []
    for a, b in ((1, 0), (1, 1), (0, 1)):
        dev = at(dh=a, dxl=b)
        n_send.append(remote(dn2.at[dev[2]], dn_in.at[x], dev))
    dn_in[x] = dn2[x]

    f_send = []
    for k in (2, 1, 3, 0):
        total_k = dkv[place(k, 0):place(k, 0) + 64, :].astype(F32)
        for d in NEAR[k]:
            cp, i = back[k, d]
            cp.wait_recv()
            total_k = total_k + near_in[i].astype(F32)
        far[k * 64:(k + 1) * 64, :] = total_k.astype(BF16)
        for dh in (0, 1):
            if (k, dh) != (0, 0):
                f_send.append(remote(far.at[pl.ds(k * 64 + dh * 32, 32), :], far_in.at[dh, k],
                                     at(dz=4 * k, dh=dh)))
    far_in[0, 0] = far[0:32, :]

    z_send = []
    for part in range(2):
        for cp in w_send[part]:
            cp.wait_recv()
        half = slice(8 * part, 8 * part + 8)
        wsum = dw_in[half, 0].astype(F32)
        for j in range(1, 4):
            wsum = wsum + dw_in[half, j].astype(F32)
        dw1[half] = wsum.astype(BF16)
        for i in range(8 * part, 8 * part + 8):
            if ZORDER[i]:
                z_send.append(remote(dw1.at[i], dw2.at[i], at(dz=ZORDER[i])))
    dw2[15] = dw1[15]

    for cp in n_send:
        cp.wait_recv()
    nsum = dn_in[0].astype(F32)
    for j in range(1, 4):
        nsum = nsum + dn_in[j].astype(F32)
    own_rows = rows_of(tp, 16)
    d_target[own_rows, :] = normed_back(tg[own_rows, :], tgn[...], nsum).astype(BF16)
    own_t = d_target.at[own_rows, :]
    t_send = {}
    for a, b in ((1, 0), (1, 1), (0, 1)):
        t_send[a, b] = remote(own_t, own_t, at(dh=a, dxl=b))
    t_pair = remote(own_t, own_t, at(dc=1))
    t_fwd = []
    for a, b in ((0, 1), (1, 0), (1, 1)):
        t_send[a, b].wait_recv()
        x2 = lax.rem(xh + a, 2) * 2 + lax.rem(xl + b, 2)
        r = d_target.at[rows_of(x2 * 2 + c, 16), :]
        t_fwd.append(remote(r, r, at(dc=1)))

    for cp in f_send:
        cp.wait_recv()
    fs = []
    for dh in range(2):
        v = far_in[dh, 0].astype(F32)
        for k in range(1, 4):
            v = v + far_in[dh, k].astype(F32)
        fs.append(v)
    low = jnp.where(xh == 0, fs[0], fs[1]).astype(BF16)
    high = jnp.where(xh == 0, fs[1], fs[0]).astype(BF16)
    dkey = jnp.concatenate([low[:, :128], high[:, :128]], axis=1)
    dval = jnp.concatenate([low[:, 128:], high[:, 128:]], axis=1)
    dns = dot(dkey, wk[...], NT) + dot(dval, wv[...], NT)
    d_source[...] = normed_back(sr[...], sgn[...], dns)

    for cp in z_send:
        cp.wait_recv()
    zsum = dw2[0].astype(F32)
    for j in range(1, 16):
        zsum = zsum + dw2[j].astype(F32)
    d_w[...] = zsum
    t_pair.wait_recv()
    for cp in t_fwd:
        cp.wait_recv()
    assert count[0] <= MESSAGES
    for cp in pending:
        cp.wait_send()


def store_kernel(a, b, w, a_out, b_out, w_out, sem):
    copies = [pltpu.make_async_copy(s, d, sem.at[k])
              for k, (s, d) in enumerate(((a, a_out), (b, b_out), (w, w_out)))]
    for cp in copies:
        cp.start()
    for cp in copies:
        cp.wait()


def local(target, source, target_gain, source_gain, w_query, w_key, w_value, attended, d_attended):
    vm = pl.BlockSpec(memory_space=pltpu.VMEM)
    anywhere = pl.BlockSpec(memory_space=pltpu.HBM)
    v = pltpu.VMEM
    outs = [jax.ShapeDtypeStruct((128, 2048), BF16), jax.ShapeDtypeStruct((32, 2048), F32),
            jax.ShapeDtypeStruct((32, 128), F32)]
    results = pl.pallas_call(
        kernel,
        out_shape=outs,
        in_specs=[anywhere] * 9,
        out_specs=[vm, vm, vm],
        scratch_shapes=[
            v((128, 2048), BF16), v((32, 2048), BF16), v((2048, 128), BF16),
            v((2048, 256), BF16), v((2048, 256), BF16), v((1, 2048), F32), v((1, 2048), F32),
            v((128, 128), BF16), v((128, 128), BF16), v((2048, 128), BF16),
            v((2, 32, 256), BF16), v((1024, 256), BF16), v((2048, 128), BF16), v((2048, 128), BF16),
            v((16, 8, 128), F32), v((8, 128), F32),
            v((16, 128), F32), v((16, 16, 128), F32), v((16, 8, 2048), F32), v((16, 8, 2048), F32),
            v((1024, 2048), F32), v((1024, 2048), F32),
            v((1024, 2048), BF16), v((1024, 2048), BF16), v((128, 1024), BF16),
            v((2048, 128), F32), v((2048, 128), BF16), v((16, 128, 128), BF16),
            v((128, 2048), BF16), v((128, 2048), BF16),
            v((2048, 128), BF16), v((2048, 128), BF16), v((1024, 256), BF16),
            v((12, 64, 256), BF16), v((256, 256), BF16), v((2, 4, 32, 256), BF16),
            v((16, 4, 32, 128), BF16), v((16, 4, 32, 128), BF16), v((16, 32, 128), BF16),
            v((16, 32, 128), BF16), v((4, 2, 16, 2048), BF16), v((4, 16, 2048), BF16),
            v((4, 16, 2048), BF16), v((4, 16, 2048), BF16),
            pltpu.SemaphoreType.DMA((9,)), pltpu.SemaphoreType.DMA((MESSAGES,)),
            pltpu.SemaphoreType.DMA((MESSAGES,)),
        ],
        compiler_params=pltpu.CompilerParams(
            collective_id=0, has_side_effects=True, vmem_limit_bytes=52 * 1024 * 1024),
        name="step",
    )(*(pltpu.with_memory_space_constraint(array, pltpu.HBM) for array in (
        target, source, target_gain.reshape(1, 2048), source_gain.reshape(1, 2048),
        w_query, w_key, w_value, attended, d_attended)))
    return tuple(pl.pallas_call(
        store_kernel, out_shape=outs, in_specs=[vm] * 3, out_specs=[anywhere] * 3,
        scratch_shapes=[pltpu.SemaphoreType.DMA((3,))],
        compiler_params=pltpu.CompilerParams(vmem_limit_bytes=4 * 1024 * 1024),
        name="store")(*results))


def solution(mesh):
    fine = Mesh(mesh.devices.reshape(NZ, NY, NX, NC), ("z", "y", "x", "c"))
    sp = ("z", "y")
    tp = ("x", "c")
    both = ("z", "y", "x", "c")
    placed = (P(sp, None), P(both, None), P(), P(), P(None, tp), P(), P(), P(sp, tp), P(sp, tp))
    return jax.shard_map(
        local, mesh=fine, in_specs=placed,
        out_specs=(P(sp, None), P(both, None), P(sp, tp)), check_vma=False)
```

```python
import jax
import jax.numpy as jnp
from jax import lax
from jax.experimental import pallas as pl
from jax.experimental.pallas import tpu as pltpu
from jax.sharding import Mesh
from jax.sharding import PartitionSpec as P

HD = 128
EPS = 1e-06
SCALE = HD ** (-0.5)
LOG2E = 1.4426950408889634
NZ, NY, NX, NC = 16, 4, 4, 2
MESH = pl.DeviceIdType.MESH
F32 = jnp.float32
BF16 = jnp.bfloat16
NT = (((1,), (1,)), ((), ()))
NN = (((1,), (0,)), ((), ()))
MESSAGES = 160
EARLY = 8
BASE = {0: 0, 1: 320, 3: 576, 2: 832}
SIZE = {0: 320, 1: 256, 3: 256, 2: 192}
NEAR = {0: (1, -1, 2, -2), 1: (-2, 1, -1), 3: (2, 1, -1), 2: (1, -1)}
ZORDER = (8, 7, 9, 6, 10, 5, 11, 4, 12, 3, 13, 2, 14, 1, 15, 0)


def dot(a, b, dims=NN):
    return lax.dot_general(a, b, dims, preferred_element_type=F32)


def place(k, d):
    if d == 0:
        slot = 0
    elif d == -1:
        slot = 1
    elif d == 1:
        slot = 2
    elif d == -2:
        slot = 3
    else:
        slot = 4 if k == 0 else 3
    return BASE[k] + 64 * slot


def normed(matrix, gain):
    wide = matrix.astype(F32)
    inverse = lax.rsqrt(jnp.mean(wide * wide, axis=-1, keepdims=True) + EPS)
    return (wide * inverse * gain).astype(BF16)


def normed_back(matrix, gain, cotangent):
    wide = matrix.astype(F32)
    inverse = lax.rsqrt(jnp.mean(wide * wide, axis=-1, keepdims=True) + EPS)
    scaled = cotangent * gain
    along = jnp.mean(scaled * wide, axis=-1, keepdims=True)
    return scaled * inverse - wide * (inverse * inverse * inverse * along)


def kernel(target, source, tgain, sgain, w_query, w_key, w_value, attended, d_attended,
           d_target, d_source, d_w,
           tg, sr, wq, wk, wv, tgn, sgn, att, dat, nt_t, nt_r, kv_own, kv, q, do, dl, own_dl,
           st, st_all, mg, lg, e_scr, u_scr, pt, ut, kt, dqf, frow, dq, dq_in, q_t, do_t, q2, do2, dkv, near_in,
           far, far_in, dw, dw_in, dw1, dw2, dn, dn_pair, dn2, dn_in,
           load_sem, send_sem, recv_sem):
    z = lax.axis_index("z")
    y = lax.axis_index("y")
    x = lax.axis_index("x")
    c = lax.axis_index("c")
    xh = x // 2
    xl = lax.rem(x, 2)
    mine = y * 4 + xl * 2 + c
    tp = x * 2 + c

    def zmod(v):
        return lax.rem(v + NZ, NZ)

    def at(dz=0, dy=0, dxl=0, dc=0, dh=0):
        x2 = lax.rem(xh + dh, 2) * 2 + lax.rem(xl + dxl, 2)
        return (zmod(z + dz), lax.rem(y + dy, NY), x2, lax.rem(c + dc, 2))

    def block(dy, dxl, dc):
        return lax.rem(y + dy + NY, NY) * 4 + lax.rem(xl + dxl, 2) * 2 + lax.rem(c + dc, 2)

    def rows_of(j, n=128):
        return pl.ds(pl.multiple_of(j * n, n), n)

    count = [0]
    pending = []

    def remote(src, dst, dev):
        k = count[0]
        count[0] += 1
        cp = pltpu.make_async_remote_copy(
            src_ref=src, dst_ref=dst, send_sem=send_sem.at[k], recv_sem=recv_sem.at[k],
            device_id=dev, device_id_type=MESH)
        cp.start()
        pending.append(cp)
        return cp

    loads = []
    for k, (a, b) in enumerate(((source, sr), (sgain, sgn), (w_key, wk), (w_value, wv),
                                (target, tg), (tgain, tgn), (w_query, wq),
                                (d_attended, dat), (attended, att))):
        cp = pltpu.make_async_copy(a, b, load_sem.at[k])
        cp.start()
        loads.append(cp)

    offs = [(dy, dx, dc) for dy in (2, 1, 3, 0) for dx in (1, 0) for dc in (1, 0)][:-1]
    peers = [at(dy=a, dxl=b, dc=d) for a, b, d in offs]
    peers += [at(dz=k) for k in range(1, 16)]
    peers += [at(dz=k, dh=1) for k in (4, 8, 12)]
    peers += [at(dh=1, dxl=a, dc=b) for a in (0, 1) for b in (0, 1)]
    barrier = pltpu.get_barrier_semaphore()
    for d in peers:
        pl.semaphore_signal(barrier, inc=1, device_id=d, device_id_type=MESH)

    for k in range(4):
        loads[k].wait()
    ns = normed(sr[...], sgn[...])
    key = dot(ns, wk[...]).astype(BF16)
    value = dot(ns, wv[...]).astype(BF16)
    kv_own[0] = jnp.concatenate([key[:, :128], value[:, :128]], axis=1)
    kv_own[1] = jnp.concatenate([key[:, 128:], value[:, 128:]], axis=1)
    pl.semaphore_wait(barrier, len(peers))

    g1 = {}
    for k, dh in ((0, 1), (2, 0), (2, 1), (1, 0), (1, 1), (3, 0), (3, 1)):
        slot = (4 - k) % 4
        g1[slot, dh] = remote(kv_own.at[lax.rem(xh + dh, 2)],
                              kv.at[pl.ds(place(slot, 0) + dh * 32, 32), :], at(dz=4 * k, dh=dh))
    kv[0:32, :] = kv_own[xh]

    for k in range(4, 9):
        loads[k].wait()
    nt = normed(tg[...], tgn[...])
    q[rows_of(mine), :] = dot(nt, wq[...]).astype(BF16)
    do[rows_of(mine), :] = dat[...]
    chips = ((2, 0), (2, 1), (1, 0), (3, 0), (1, 1), (3, 1), (0, 1))
    own_q = q.at[rows_of(mine), :]
    own_do = do.at[rows_of(mine), :]
    q_send = {o: remote(own_q, own_q, at(dy=o[0], dxl=o[1])) for o in chips}
    q_pair = remote(own_q, own_q, at(dc=1))
    prod = dat[...].astype(F32) * att[...].astype(F32)
    delta = jnp.sum(jnp.transpose(prod), axis=0, keepdims=True).astype(BF16).astype(F32)
    own_dl[...] = jnp.broadcast_to(delta, (8, 128))
    dl[mine] = own_dl[...]
    do_send = {o: remote(own_do, own_do, at(dy=o[0], dxl=o[1])) for o in chips}
    do_pair = remote(own_do, own_do, at(dc=1))
    dl_send = [remote(own_dl, dl.at[mine], at(dy=a, dxl=b, dc=d)) for a, b, d in offs]
    nt_t[...] = jnp.transpose(nt)
    for i in range(16):
        nt_r[i * 128:(i + 1) * 128, :] = nt_t[rows_of(zmod(z + ZORDER[i])), :]

    near = {}

    def forward(k):
        src = kv.at[pl.ds(place(k, 0), 64), :]
        for d in NEAR[k]:
            near[k, d] = remote(src, kv.at[pl.ds(place(k, d), 64), :], at(dz=d))

    def pass_on(sends, array):
        out = []
        for dy, dx in ((0, 1), (1, 0), (3, 0), (1, 1), (3, 1), (2, 0), (2, 1)):
            sends[dy, dx].wait_recv()
            r = array.at[rows_of(block(-dy, dx, 0)), :]
            out.append(remote(r, r, at(dc=1)))
        return out

    def arrived(k):
        for d in NEAR[k]:
            near[k, d].wait_recv()

    def far_arrived(k):
        for dh in (0, 1):
            if (k, dh) != (0, 0):
                g1[k, dh].wait_recv()

    def scores(k):
        base, size = BASE[k], SIZE[k]

        def pair(p):
            cols = slice(p * 256, (p + 1) * 256)
            s = dot(kv[base:base + size, :128], q_t[:, cols])
            for i in range(size // 64):
                t = s[i * 64:(i + 1) * 64].reshape(8, 8, 256) * (SCALE * LOG2E)
                m = jnp.max(t, axis=0)
                e = jnp.exp2(t - m[None])
                n = base // 64 + i
                mg[n, :, cols] = m
                lg[n, :, cols] = jnp.sum(e, axis=0)
                e_scr[base + i * 64:base + (i + 1) * 64, cols] = e.reshape(64, 256)

        for p in range(8):
            pair(p)

    def weights_back(k):
        base, size = BASE[k], SIZE[k]

        def pair(p):
            cols = slice(p * 256, (p + 1) * 256)
            g = dot(kv[base:base + size, 128:], do_t[:, cols])
            drow = jnp.concatenate([dl[2 * p, 0:1, :], dl[2 * p + 1, 0:1, :]], axis=1)
            u_scr[base:base + size, cols] = e_scr[base:base + size, cols] * (g - drow)

        for p in range(8):
            pair(p)

    far_arrived(0)
    forward(0)
    q_fwd = pass_on(q_send, q)
    for k in (1, 3):
        far_arrived(k)
        forward(k)
    q_pair.wait_recv()
    for cp in q_fwd:
        cp.wait_recv()
    q_t[...] = jnp.transpose(q[...])
    arrived(0)
    scores(0)
    do_fwd = pass_on(do_send, do)
    far_arrived(2)
    forward(2)
    arrived(1)
    scores(1)
    arrived(3)
    scores(3)
    do_pair.wait_recv()
    for cp in do_fwd + dl_send:
        cp.wait_recv()
    do_t[...] = jnp.transpose(do[...])
    weights_back(0)
    weights_back(1)
    kt[:, :832] = jnp.transpose(kv[:832, :128])
    arrived(2)
    scores(2)
    top8 = jnp.max(mg[...], axis=0)
    top1 = jnp.max(top8, axis=0, keepdims=True)
    tot = lg[0] * jnp.exp2(mg[0] - top1)
    for i in range(1, 16):
        tot = tot + lg[i] * jnp.exp2(mg[i] - top1)
    lse = top1 + jnp.log(jnp.sum(tot, axis=0, keepdims=True)) * LOG2E
    for j in range(16):
        st[j:j + 1, :] = lse[:, j * 128:(j + 1) * 128]
    stats = [remote(st, st_all.at[mine], at(dy=a, dxl=b, dc=d)) for a, b, d in offs]
    st_all[mine] = st[...]
    for i in range(16):
        mg[i] = jnp.exp2(mg[i] - lse)
    kt[:, 832:] = jnp.transpose(kv[832:, :128])

    def grads(dy, dx):
        p = lax.rem(y + dy, NY) * 2 + lax.rem(xl + dx, 2)
        cols = rows_of(p, 256)
        drow = jnp.concatenate([dl[2 * p, 0:1, :], dl[2 * p + 1, 0:1, :]], axis=1)
        dot_p = do_t[:, cols]
        for k in (0, 1, 3, 2):
            base, size = BASE[k], SIZE[k]
            if k in (3, 2):
                g = dot(kv[base:base + size, 128:], dot_p) - drow
            for i in range(size // 64):
                n = base // 64 + i
                r = slice(n * 64, (n + 1) * 64)
                f = mg[n, :, cols][None]
                w = e_scr[r, cols].reshape(8, 8, 256) * f
                pt[r, cols] = w.reshape(64, 256).astype(BF16)
                if k in (3, 2):
                    u = w * g[i * 64:(i + 1) * 64].reshape(8, 8, 256)
                else:
                    u = u_scr[r, cols].reshape(8, 8, 256) * f
                ut[r, cols] = u.reshape(64, 256).astype(BF16)
        return cols, dot(kt[...], ut[:, cols]) * SCALE

    order = ((2, 1), (2, 0), (1, 1), (3, 1), (1, 0), (3, 0), (0, 1), (0, 0))
    dq_send = []

    def dq_out(cols, value, dy, dx):
        dq[cols, :] = jnp.transpose(value * frow[0:1, cols]).astype(BF16)
        for dc in (1, 0):
            if (dy, dx, dc) != (0, 0, 0):
                dq_send.append(remote(dq.at[rows_of(block(dy, dx, dc)), :], dq_in.at[mine],
                                      at(dy=dy, dxl=dx, dc=dc)))

    held = []
    for dy, dx in order[:EARLY]:
        cols, value = grads(dy, dx)
        dqf[:, cols] = value
        held.append((cols, dy, dx))
    for cp in stats:
        cp.wait_recv()
    top = jnp.max(st_all[...], axis=0)
    total = jnp.zeros((16, 128), F32)
    for j in range(16):
        total = total + jnp.exp2(st_all[j] - top)
    factor = jnp.exp2(st[...] - (top + jnp.log(total) * LOG2E))
    factor_t = jnp.transpose(jnp.concatenate([factor, jnp.zeros((112, 128), F32)], axis=0))
    for j in range(16):
        frow[0:1, j * 128:(j + 1) * 128] = factor[j:j + 1, :]
    for cols, dy, dx in held:
        dq_out(cols, dqf[:, cols], dy, dx)
    for dy, dx in order[EARLY:]:
        cols, value = grads(dy, dx)
        dq_out(cols, value, dy, dx)
    dq_in[mine] = dq[rows_of(mine), :]
    for j in range(16):
        r = slice(j * 128, (j + 1) * 128)
        f = factor_t[:, j:j + 1]
        q2[r, :] = (q[r, :].astype(F32) * f).astype(BF16)
        do2[r, :] = (do[r, :].astype(F32) * f).astype(BF16)
    back = {}
    index = 0
    for k in (2, 1, 3, 0):
        r = slice(BASE[k], BASE[k] + SIZE[k])
        dk = dot(ut[r, :], q2[...]) * SCALE
        dv = dot(pt[r, :], do2[...])
        dkv[r, :] = jnp.concatenate([dk, dv], axis=1).astype(BF16)
        for d in NEAR[k]:
            back[k, d] = (remote(dkv.at[pl.ds(place(k, d), 64), :], near_in.at[index], at(dz=-d)),
                          index)
            index += 1

    for cp in dq_send:
        cp.wait_recv()
    acc = dq_in[0].astype(F32)
    for j in range(1, 16):
        acc = acc + dq_in[j].astype(F32)
    dqb = acc.astype(BF16)
    w_all = dot(nt_r[...], dqb).astype(BF16)
    dn_all = dot(dqb, wq[...], NT).astype(BF16)
    dw[...] = w_all.reshape(16, 4, 32, 128)
    w_send = ([], [])
    for part in range(2):
        for d in (2, 1, 3):
            some = pl.ds(8 * part, 8)
            w_send[part].append(remote(dw.at[some, lax.rem(y + d, NY)], dw_in.at[some, y],
                                       at(dy=d)))
        if part == 0:
            dn[...] = dn_all.reshape(4, 2, 16, 2048)
            pair_send = remote(dn.at[:, lax.rem(c + 1, 2)], dn_pair, at(dc=1))
    dw_in[:, y] = dw[:, y]

    pair_send.wait_recv()
    dn2[...] = (dn[:, c].astype(F32) + dn_pair[...].astype(F32)).astype(BF16)
    n_send = []
    for a, b in ((1, 0), (1, 1), (0, 1)):
        dev = at(dh=a, dxl=b)
        n_send.append(remote(dn2.at[dev[2]], dn_in.at[x], dev))
    dn_in[x] = dn2[x]

    f_send = []
    for k in (2, 1, 3, 0):
        total_k = dkv[place(k, 0):place(k, 0) + 64, :].astype(F32)
        for d in NEAR[k]:
            cp, i = back[k, d]
            cp.wait_recv()
            total_k = total_k + near_in[i].astype(F32)
        far[k * 64:(k + 1) * 64, :] = total_k.astype(BF16)
        for dh in (0, 1):
            if (k, dh) != (0, 0):
                f_send.append(remote(far.at[pl.ds(k * 64 + dh * 32, 32), :], far_in.at[dh, k],
                                     at(dz=4 * k, dh=dh)))
    far_in[0, 0] = far[0:32, :]

    z_send = []

    def z_part(part):
        for cp in w_send[part]:
            cp.wait_recv()
        half = slice(8 * part, 8 * part + 8)
        wsum = dw_in[half, 0].astype(F32)
        for j in range(1, 4):
            wsum = wsum + dw_in[half, j].astype(F32)
        dw1[half] = wsum.astype(BF16)
        for i in range(8 * part, 8 * part + 8):
            if ZORDER[i]:
                z_send.append(remote(dw1.at[i], dw2.at[i], at(dz=ZORDER[i])))

    z_part(0)
    z_part(1)
    dw2[15] = dw1[15]

    for cp in n_send:
        cp.wait_recv()
    nsum = dn_in[0].astype(F32)
    for j in range(1, 4):
        nsum = nsum + dn_in[j].astype(F32)
    own_rows = rows_of(tp, 16)
    d_target[own_rows, :] = normed_back(tg[own_rows, :], tgn[...], nsum).astype(BF16)
    own_t = d_target.at[own_rows, :]
    t_send = {}
    for a, b in ((1, 0), (1, 1), (0, 1)):
        t_send[a, b] = remote(own_t, own_t, at(dh=a, dxl=b))
    t_pair = remote(own_t, own_t, at(dc=1))
    t_fwd = []
    for a, b in ((0, 1), (1, 0), (1, 1)):
        t_send[a, b].wait_recv()
        x2 = lax.rem(xh + a, 2) * 2 + lax.rem(xl + b, 2)
        r = d_target.at[rows_of(x2 * 2 + c, 16), :]
        t_fwd.append(remote(r, r, at(dc=1)))

    for cp in f_send:
        cp.wait_recv()
    fs = []
    for dh in range(2):
        v = far_in[dh, 0].astype(F32)
        for k in range(1, 4):
            v = v + far_in[dh, k].astype(F32)
        fs.append(v)
    low = jnp.where(xh == 0, fs[0], fs[1]).astype(BF16)
    high = jnp.where(xh == 0, fs[1], fs[0]).astype(BF16)
    dkey = jnp.concatenate([low[:, :128], high[:, :128]], axis=1)
    dval = jnp.concatenate([low[:, 128:], high[:, 128:]], axis=1)
    dns = dot(dkey, wk[...], NT) + dot(dval, wv[...], NT)
    d_source[...] = normed_back(sr[...], sgn[...], dns)

    for cp in z_send:
        cp.wait_recv()
    zsum = dw2[0].astype(F32)
    for j in range(1, 16):
        zsum = zsum + dw2[j].astype(F32)
    d_w[...] = zsum
    t_pair.wait_recv()
    for cp in t_fwd:
        cp.wait_recv()
    assert count[0] <= MESSAGES
    for cp in pending:
        cp.wait_send()


def store_kernel(a, b, w, a_out, b_out, w_out, sem):
    copies = [pltpu.make_async_copy(s, d, sem.at[k])
              for k, (s, d) in enumerate(((a, a_out), (b, b_out), (w, w_out)))]
    for cp in copies:
        cp.start()
    for cp in copies:
        cp.wait()


def local(target, source, target_gain, source_gain, w_query, w_key, w_value, attended, d_attended):
    vm = pl.BlockSpec(memory_space=pltpu.VMEM)
    anywhere = pl.BlockSpec(memory_space=pltpu.HBM)
    v = pltpu.VMEM
    outs = [jax.ShapeDtypeStruct((128, 2048), BF16), jax.ShapeDtypeStruct((32, 2048), F32),
            jax.ShapeDtypeStruct((32, 128), F32)]
    results = pl.pallas_call(
        kernel,
        out_shape=outs,
        in_specs=[anywhere] * 9,
        out_specs=[vm, vm, vm],
        scratch_shapes=[
            v((128, 2048), BF16), v((32, 2048), BF16), v((2048, 128), BF16),
            v((2048, 256), BF16), v((2048, 256), BF16), v((1, 2048), F32), v((1, 2048), F32),
            v((128, 128), BF16), v((128, 128), BF16), v((2048, 128), BF16), v((2048, 128), BF16),
            v((2, 32, 256), BF16), v((1024, 256), BF16), v((2048, 128), BF16), v((2048, 128), BF16),
            v((16, 8, 128), F32), v((8, 128), F32),
            v((16, 128), F32), v((16, 16, 128), F32), v((16, 8, 2048), F32), v((16, 8, 2048), F32),
            v((1024, 2048), F32), v((1024, 2048), F32),
            v((1024, 2048), BF16), v((1024, 2048), BF16), v((128, 1024), BF16),
            v((128, 2048), F32), v((8, 2048), F32), v((2048, 128), BF16),
            v((16, 128, 128), BF16),
            v((128, 2048), BF16), v((128, 2048), BF16),
            v((2048, 128), BF16), v((2048, 128), BF16), v((1024, 256), BF16),
            v((12, 64, 256), BF16), v((256, 256), BF16), v((2, 4, 32, 256), BF16),
            v((16, 4, 32, 128), BF16), v((16, 4, 32, 128), BF16), v((16, 32, 128), BF16),
            v((16, 32, 128), BF16), v((4, 2, 16, 2048), BF16), v((4, 16, 2048), BF16),
            v((4, 16, 2048), BF16), v((4, 16, 2048), BF16),
            pltpu.SemaphoreType.DMA((9,)), pltpu.SemaphoreType.DMA((MESSAGES,)),
            pltpu.SemaphoreType.DMA((MESSAGES,)),
        ],
        compiler_params=pltpu.CompilerParams(
            collective_id=0, has_side_effects=True, vmem_limit_bytes=52 * 1024 * 1024),
        name="step",
    )(*(pltpu.with_memory_space_constraint(array, pltpu.HBM) for array in (
        target, source, target_gain.reshape(1, 2048), source_gain.reshape(1, 2048),
        w_query, w_key, w_value, attended, d_attended)))
    return tuple(pl.pallas_call(
        store_kernel, out_shape=outs, in_specs=[vm] * 3, out_specs=[anywhere] * 3,
        scratch_shapes=[pltpu.SemaphoreType.DMA((3,))],
        compiler_params=pltpu.CompilerParams(vmem_limit_bytes=4 * 1024 * 1024),
        name="store")(*results))


def solution(mesh):
    fine = Mesh(mesh.devices.reshape(NZ, NY, NX, NC), ("z", "y", "x", "c"))
    sp = ("z", "y")
    tp = ("x", "c")
    both = ("z", "y", "x", "c")
    placed = (P(sp, None), P(both, None), P(), P(), P(None, tp), P(), P(), P(sp, tp), P(sp, tp))
    return jax.shard_map(
        local, mesh=fine, in_specs=placed,
        out_specs=(P(sp, None), P(both, None), P(sp, tp)), check_vma=False)
```

```python
import jax
import jax.numpy as jnp
from jax import lax
from jax.experimental import pallas as pl
from jax.experimental.pallas import tpu as pltpu
from jax.sharding import Mesh
from jax.sharding import PartitionSpec as P

HD = 128
EPS = 1e-06
SCALE = HD ** (-0.5)
LOG2E = 1.4426950408889634
NZ, NY, NX, NC = 16, 4, 4, 2
MESH = pl.DeviceIdType.MESH
F32 = jnp.float32
BF16 = jnp.bfloat16
NT = (((1,), (1,)), ((), ()))
NN = (((1,), (0,)), ((), ()))
MESSAGES = 176
EARLY = 8
BASE = {0: 0, 1: 320, 3: 576, 2: 832}
SIZE = {0: 320, 1: 256, 3: 256, 2: 192}
NEAR = {0: (1, -1, 2, -2), 1: (-2, 1, -1), 3: (2, 1, -1), 2: (1, -1)}
ZORDER = (8, 7, 9, 6, 10, 5, 11, 4, 12, 3, 13, 2, 14, 1, 15, 0)


def dot(a, b, dims=NN):
    return lax.dot_general(a, b, dims, preferred_element_type=F32)


def place(k, d):
    if d == 0:
        slot = 0
    elif d == -1:
        slot = 1
    elif d == 1:
        slot = 2
    elif d == -2:
        slot = 3
    else:
        slot = 4 if k == 0 else 3
    return BASE[k] + 64 * slot


def normed(matrix, gain):
    wide = matrix.astype(F32)
    inverse = lax.rsqrt(jnp.mean(wide * wide, axis=-1, keepdims=True) + EPS)
    return (wide * inverse * gain).astype(BF16)


def normed_back(matrix, gain, cotangent):
    wide = matrix.astype(F32)
    inverse = lax.rsqrt(jnp.mean(wide * wide, axis=-1, keepdims=True) + EPS)
    scaled = cotangent * gain
    along = jnp.mean(scaled * wide, axis=-1, keepdims=True)
    return scaled * inverse - wide * (inverse * inverse * inverse * along)


def kernel(target, source, tgain, sgain, w_query, w_key, w_value, attended, d_attended,
           d_target, d_source, d_w,
           tg, sr, wq, wk, wv, tgn, sgn, att, dat, nt_t, nt_r, k_own, v_own, ks, vs, q, do, dl, own_dl,
           st, st_all, mg, lg, e_scr, u_scr, pt, ut, kt, dqf, frow, dq, dq_in, q_t, do_t, q2, do2, dkv, near_in,
           far, far_in, dw, dw_in, dw1, dw2, dn, dn_pair, dn2, dn_in,
           load_sem, send_sem, recv_sem):
    z = lax.axis_index("z")
    y = lax.axis_index("y")
    x = lax.axis_index("x")
    c = lax.axis_index("c")
    xh = x // 2
    xl = lax.rem(x, 2)
    mine = y * 4 + xl * 2 + c
    tp = x * 2 + c

    def zmod(v):
        return lax.rem(v + NZ, NZ)

    def at(dz=0, dy=0, dxl=0, dc=0, dh=0):
        x2 = lax.rem(xh + dh, 2) * 2 + lax.rem(xl + dxl, 2)
        return (zmod(z + dz), lax.rem(y + dy, NY), x2, lax.rem(c + dc, 2))

    def block(dy, dxl, dc):
        return lax.rem(y + dy + NY, NY) * 4 + lax.rem(xl + dxl, 2) * 2 + lax.rem(c + dc, 2)

    def rows_of(j, n=128):
        return pl.ds(pl.multiple_of(j * n, n), n)

    count = [0]
    pending = []

    def remote(src, dst, dev):
        k = count[0]
        count[0] += 1
        cp = pltpu.make_async_remote_copy(
            src_ref=src, dst_ref=dst, send_sem=send_sem.at[k], recv_sem=recv_sem.at[k],
            device_id=dev, device_id_type=MESH)
        cp.start()
        pending.append(cp)
        return cp

    loads = []
    for k, (a, b) in enumerate(((source, sr), (sgain, sgn), (w_key, wk), (w_value, wv),
                                (target, tg), (tgain, tgn), (w_query, wq),
                                (d_attended, dat), (attended, att))):
        cp = pltpu.make_async_copy(a, b, load_sem.at[k])
        if k < 4:
            cp.start()
        loads.append(cp)

    offs = [(dy, dx, dc) for dy in (2, 1, 3, 0) for dx in (1, 0) for dc in (1, 0)][:-1]
    peers = [at(dy=a, dxl=b, dc=d) for a, b, d in offs]
    peers += [at(dz=k) for k in range(1, 16)]
    peers += [at(dz=k, dh=1) for k in (4, 8, 12)]
    peers += [at(dh=1, dxl=a, dc=b) for a in (0, 1) for b in (0, 1)]
    barrier = pltpu.get_barrier_semaphore()
    for d in peers:
        pl.semaphore_signal(barrier, inc=1, device_id=d, device_id_type=MESH)

    for k in range(4):
        loads[k].wait()
    for cp in loads[4:]:
        cp.start()
    ns = normed(sr[...], sgn[...])
    key = dot(ns, wk[...]).astype(BF16)
    value = dot(ns, wv[...]).astype(BF16)
    for i in range(2):
        k_own[i] = key[:, i * 128:(i + 1) * 128]
        v_own[i] = value[:, i * 128:(i + 1) * 128]
    pl.semaphore_wait(barrier, len(peers))

    g1 = {}
    for which, own, full in ((0, k_own, ks), (1, v_own, vs)):
        for k, dh in ((0, 1), (2, 0), (2, 1), (1, 0), (1, 1), (3, 0), (3, 1)):
            slot = (4 - k) % 4
            g1[which, slot, dh] = remote(own.at[lax.rem(xh + dh, 2)],
                                         full.at[pl.ds(place(slot, 0) + dh * 32, 32), :],
                                         at(dz=4 * k, dh=dh))
        full[0:32, :] = own[xh]

    for k in range(4, 9):
        loads[k].wait()
    nt = normed(tg[...], tgn[...])
    q[rows_of(mine), :] = dot(nt, wq[...]).astype(BF16)
    do[rows_of(mine), :] = dat[...]
    chips = ((2, 0), (2, 1), (1, 0), (3, 0), (1, 1), (3, 1), (0, 1))
    own_q = q.at[rows_of(mine), :]
    own_do = do.at[rows_of(mine), :]
    q_send = {o: remote(own_q, own_q, at(dy=o[0], dxl=o[1])) for o in chips}
    q_pair = remote(own_q, own_q, at(dc=1))
    prod = dat[...].astype(F32) * att[...].astype(F32)
    delta = jnp.sum(jnp.transpose(prod), axis=0, keepdims=True).astype(BF16).astype(F32)
    own_dl[...] = jnp.broadcast_to(delta, (8, 128))
    dl[mine] = own_dl[...]
    do_send = {o: remote(own_do, own_do, at(dy=o[0], dxl=o[1])) for o in chips}
    do_pair = remote(own_do, own_do, at(dc=1))
    dl_send = [remote(own_dl, dl.at[mine], at(dy=a, dxl=b, dc=d)) for a, b, d in offs]
    nt_t[...] = jnp.transpose(nt)
    for i in range(16):
        nt_r[i * 128:(i + 1) * 128, :] = nt_t[rows_of(zmod(z + ZORDER[i])), :]

    near = {}

    def forward(which, k):
        full = vs if which else ks
        src = full.at[pl.ds(place(k, 0), 64), :]
        for d in NEAR[k]:
            near[which, k, d] = remote(src, full.at[pl.ds(place(k, d), 64), :], at(dz=d))

    def pass_on(sends, array):
        out = []
        for dy, dx in ((0, 1), (1, 0), (3, 0), (1, 1), (3, 1), (2, 0), (2, 1)):
            sends[dy, dx].wait_recv()
            r = array.at[rows_of(block(-dy, dx, 0)), :]
            out.append(remote(r, r, at(dc=1)))
        return out

    def arrived(which, k):
        for d in NEAR[k]:
            near[which, k, d].wait_recv()

    def relay(which, k):
        for dh in (0, 1):
            if (k, dh) != (0, 0):
                g1[which, k, dh].wait_recv()
        forward(which, k)

    def scores(k):
        base, size = BASE[k], SIZE[k]

        def pair(p):
            cols = slice(p * 256, (p + 1) * 256)
            s = dot(ks[base:base + size, :], q_t[:, cols])
            for i in range(size // 64):
                t = s[i * 64:(i + 1) * 64].reshape(8, 8, 256) * (SCALE * LOG2E)
                m = jnp.max(t, axis=0)
                e = jnp.exp2(t - m[None])
                n = base // 64 + i
                mg[n, :, cols] = m
                lg[n, :, cols] = jnp.sum(e, axis=0)
                e_scr[base + i * 64:base + (i + 1) * 64, cols] = e.reshape(64, 256)

        for p in range(8):
            pair(p)

    def weights_back(k):
        base, size = BASE[k], SIZE[k]

        def pair(p):
            cols = slice(p * 256, (p + 1) * 256)
            g = dot(vs[base:base + size, :], do_t[:, cols])
            drow = jnp.concatenate([dl[2 * p, 0:1, :], dl[2 * p + 1, 0:1, :]], axis=1)
            u_scr[base:base + size, cols] = e_scr[base:base + size, cols] * (g - drow)

        for p in range(8):
            pair(p)

    relay(0, 0)
    q_fwd = pass_on(q_send, q)
    relay(0, 1)
    relay(0, 3)
    relay(1, 0)
    q_pair.wait_recv()
    for cp in q_fwd:
        cp.wait_recv()
    q_t[...] = jnp.transpose(q[...])
    arrived(0, 0)
    scores(0)
    relay(0, 2)
    do_fwd = pass_on(do_send, do)
    relay(1, 1)
    relay(1, 3)
    arrived(0, 1)
    scores(1)
    arrived(0, 3)
    scores(3)
    relay(1, 2)
    arrived(0, 2)
    scores(2)
    top8 = jnp.max(mg[...], axis=0)
    top1 = jnp.max(top8, axis=0, keepdims=True)
    tot = lg[0] * jnp.exp2(mg[0] - top1)
    for i in range(1, 16):
        tot = tot + lg[i] * jnp.exp2(mg[i] - top1)
    lse = top1 + jnp.log(jnp.sum(tot, axis=0, keepdims=True)) * LOG2E
    for j in range(16):
        st[j:j + 1, :] = lse[:, j * 128:(j + 1) * 128]
    stats = [remote(st, st_all.at[mine], at(dy=a, dxl=b, dc=d)) for a, b, d in offs]
    st_all[mine] = st[...]
    for i in range(16):
        mg[i] = jnp.exp2(mg[i] - lse)
    kt[...] = jnp.transpose(ks[...])
    do_pair.wait_recv()
    for cp in do_fwd + dl_send:
        cp.wait_recv()
    do_t[...] = jnp.transpose(do[...])
    for k in (0, 1, 3):
        arrived(1, k)
        weights_back(k)
    arrived(1, 2)

    def grads(dy, dx):
        p = lax.rem(y + dy, NY) * 2 + lax.rem(xl + dx, 2)
        cols = rows_of(p, 256)
        drow = jnp.concatenate([dl[2 * p, 0:1, :], dl[2 * p + 1, 0:1, :]], axis=1)
        dot_p = do_t[:, cols]
        for k in (0, 1, 3, 2):
            base, size = BASE[k], SIZE[k]
            if k == 2:
                g = dot(vs[base:base + size, :], dot_p) - drow
            for i in range(size // 64):
                n = base // 64 + i
                r = slice(n * 64, (n + 1) * 64)
                f = mg[n, :, cols][None]
                w = e_scr[r, cols].reshape(8, 8, 256) * f
                pt[r, cols] = w.reshape(64, 256).astype(BF16)
                if k == 2:
                    u = w * g[i * 64:(i + 1) * 64].reshape(8, 8, 256)
                else:
                    u = u_scr[r, cols].reshape(8, 8, 256) * f
                ut[r, cols] = u.reshape(64, 256).astype(BF16)
        return cols, dot(kt[...], ut[:, cols]) * SCALE

    order = ((2, 1), (2, 0), (1, 1), (3, 1), (1, 0), (3, 0), (0, 1), (0, 0))
    dq_send = []

    def dq_out(cols, value, dy, dx):
        dq[cols, :] = jnp.transpose(value * frow[0:1, cols]).astype(BF16)
        for dc in (1, 0):
            if (dy, dx, dc) != (0, 0, 0):
                dq_send.append(remote(dq.at[rows_of(block(dy, dx, dc)), :], dq_in.at[mine],
                                      at(dy=dy, dxl=dx, dc=dc)))

    held = []
    for dy, dx in order[:EARLY]:
        cols, value = grads(dy, dx)
        dqf[:, cols] = value
        held.append((cols, dy, dx))
    for cp in stats:
        cp.wait_recv()
    top = jnp.max(st_all[...], axis=0)
    total = jnp.zeros((16, 128), F32)
    for j in range(16):
        total = total + jnp.exp2(st_all[j] - top)
    factor = jnp.exp2(st[...] - (top + jnp.log(total) * LOG2E))
    factor_t = jnp.transpose(jnp.concatenate([factor, jnp.zeros((112, 128), F32)], axis=0))
    for j in range(16):
        frow[0:1, j * 128:(j + 1) * 128] = factor[j:j + 1, :]
    for cols, dy, dx in held:
        dq_out(cols, dqf[:, cols], dy, dx)
    for dy, dx in order[EARLY:]:
        cols, value = grads(dy, dx)
        dq_out(cols, value, dy, dx)
    dq_in[mine] = dq[rows_of(mine), :]
    for j in range(16):
        r = slice(j * 128, (j + 1) * 128)
        f = factor_t[:, j:j + 1]
        q2[r, :] = (q[r, :].astype(F32) * f).astype(BF16)
        do2[r, :] = (do[r, :].astype(F32) * f).astype(BF16)
    back = {}
    index = 0
    for k in (2, 1, 3, 0):
        r = slice(BASE[k], BASE[k] + SIZE[k])
        dk = dot(ut[r, :], q2[...]) * SCALE
        dv = dot(pt[r, :], do2[...])
        dkv[r, :] = jnp.concatenate([dk, dv], axis=1).astype(BF16)
        for d in NEAR[k]:
            back[k, d] = (remote(dkv.at[pl.ds(place(k, d), 64), :], near_in.at[index], at(dz=-d)),
                          index)
            index += 1

    for cp in dq_send:
        cp.wait_recv()
    acc = dq_in[0].astype(F32)
    for j in range(1, 16):
        acc = acc + dq_in[j].astype(F32)
    dqb = acc.astype(BF16)
    w_all = dot(nt_r[...], dqb).astype(BF16)
    dn_all = dot(dqb, wq[...], NT).astype(BF16)
    dw[...] = w_all.reshape(16, 4, 32, 128)
    w_send = ([], [])
    for part in range(2):
        for d in (2, 1, 3):
            some = pl.ds(8 * part, 8)
            w_send[part].append(remote(dw.at[some, lax.rem(y + d, NY)], dw_in.at[some, y],
                                       at(dy=d)))
        if part == 0:
            dn[...] = dn_all.reshape(4, 2, 16, 2048)
            pair_send = remote(dn.at[:, lax.rem(c + 1, 2)], dn_pair, at(dc=1))
    dw_in[:, y] = dw[:, y]

    pair_send.wait_recv()
    dn2[...] = (dn[:, c].astype(F32) + dn_pair[...].astype(F32)).astype(BF16)
    n_send = []
    for a, b in ((1, 0), (1, 1), (0, 1)):
        dev = at(dh=a, dxl=b)
        n_send.append(remote(dn2.at[dev[2]], dn_in.at[x], dev))
    dn_in[x] = dn2[x]

    f_send = []
    for k in (2, 1, 3, 0):
        total_k = dkv[place(k, 0):place(k, 0) + 64, :].astype(F32)
        for d in NEAR[k]:
            cp, i = back[k, d]
            cp.wait_recv()
            total_k = total_k + near_in[i].astype(F32)
        far[k * 64:(k + 1) * 64, :] = total_k.astype(BF16)
        for dh in (0, 1):
            if (k, dh) != (0, 0):
                f_send.append(remote(far.at[pl.ds(k * 64 + dh * 32, 32), :], far_in.at[dh, k],
                                     at(dz=4 * k, dh=dh)))
    far_in[0, 0] = far[0:32, :]

    z_send = []

    def z_part(part):
        for cp in w_send[part]:
            cp.wait_recv()
        half = slice(8 * part, 8 * part + 8)
        wsum = dw_in[half, 0].astype(F32)
        for j in range(1, 4):
            wsum = wsum + dw_in[half, j].astype(F32)
        dw1[half] = wsum.astype(BF16)
        for i in range(8 * part, 8 * part + 8):
            if ZORDER[i]:
                z_send.append(remote(dw1.at[i], dw2.at[i], at(dz=ZORDER[i])))

    z_part(0)
    z_part(1)
    dw2[15] = dw1[15]

    for cp in n_send:
        cp.wait_recv()
    nsum = dn_in[0].astype(F32)
    for j in range(1, 4):
        nsum = nsum + dn_in[j].astype(F32)
    own_rows = rows_of(tp, 16)
    d_target[own_rows, :] = normed_back(tg[own_rows, :], tgn[...], nsum).astype(BF16)
    own_t = d_target.at[own_rows, :]
    t_send = {}
    for a, b in ((1, 0), (1, 1), (0, 1)):
        t_send[a, b] = remote(own_t, own_t, at(dh=a, dxl=b))
    t_pair = remote(own_t, own_t, at(dc=1))
    t_fwd = []
    for a, b in ((0, 1), (1, 0), (1, 1)):
        t_send[a, b].wait_recv()
        x2 = lax.rem(xh + a, 2) * 2 + lax.rem(xl + b, 2)
        r = d_target.at[rows_of(x2 * 2 + c, 16), :]
        t_fwd.append(remote(r, r, at(dc=1)))

    for cp in f_send:
        cp.wait_recv()
    fs = []
    for dh in range(2):
        v = far_in[dh, 0].astype(F32)
        for k in range(1, 4):
            v = v + far_in[dh, k].astype(F32)
        fs.append(v)
    low = jnp.where(xh == 0, fs[0], fs[1]).astype(BF16)
    high = jnp.where(xh == 0, fs[1], fs[0]).astype(BF16)
    dkey = jnp.concatenate([low[:, :128], high[:, :128]], axis=1)
    dval = jnp.concatenate([low[:, 128:], high[:, 128:]], axis=1)
    dns = dot(dkey, wk[...], NT) + dot(dval, wv[...], NT)
    d_source[...] = normed_back(sr[...], sgn[...], dns)

    for cp in z_send:
        cp.wait_recv()
    zsum = dw2[0].astype(F32)
    for j in range(1, 16):
        zsum = zsum + dw2[j].astype(F32)
    d_w[...] = zsum
    t_pair.wait_recv()
    for cp in t_fwd:
        cp.wait_recv()
    assert count[0] <= MESSAGES
    for cp in pending:
        cp.wait_send()


def store_kernel(a, b, w, a_out, b_out, w_out, sem):
    copies = [pltpu.make_async_copy(s, d, sem.at[k])
              for k, (s, d) in enumerate(((a, a_out), (b, b_out), (w, w_out)))]
    for cp in copies:
        cp.start()
    for cp in copies:
        cp.wait()


def local(target, source, target_gain, source_gain, w_query, w_key, w_value, attended, d_attended):
    vm = pl.BlockSpec(memory_space=pltpu.VMEM)
    anywhere = pl.BlockSpec(memory_space=pltpu.HBM)
    v = pltpu.VMEM
    outs = [jax.ShapeDtypeStruct((128, 2048), BF16), jax.ShapeDtypeStruct((32, 2048), F32),
            jax.ShapeDtypeStruct((32, 128), F32)]
    results = pl.pallas_call(
        kernel,
        out_shape=outs,
        in_specs=[anywhere] * 9,
        out_specs=[vm, vm, vm],
        scratch_shapes=[
            v((128, 2048), BF16), v((32, 2048), BF16), v((2048, 128), BF16),
            v((2048, 256), BF16), v((2048, 256), BF16), v((1, 2048), F32), v((1, 2048), F32),
            v((128, 128), BF16), v((128, 128), BF16), v((2048, 128), BF16), v((2048, 128), BF16),
            v((2, 32, 128), BF16), v((2, 32, 128), BF16), v((1024, 128), BF16),
            v((1024, 128), BF16), v((2048, 128), BF16), v((2048, 128), BF16),
            v((16, 8, 128), F32), v((8, 128), F32),
            v((16, 128), F32), v((16, 16, 128), F32), v((16, 8, 2048), F32), v((16, 8, 2048), F32),
            v((1024, 2048), F32), v((1024, 2048), F32),
            v((1024, 2048), BF16), v((1024, 2048), BF16), v((128, 1024), BF16),
            v((128, 2048), F32), v((8, 2048), F32), v((2048, 128), BF16),
            v((16, 128, 128), BF16),
            v((128, 2048), BF16), v((128, 2048), BF16),
            v((2048, 128), BF16), v((2048, 128), BF16), v((1024, 256), BF16),
            v((12, 64, 256), BF16), v((256, 256), BF16), v((2, 4, 32, 256), BF16),
            v((16, 4, 32, 128), BF16), v((16, 4, 32, 128), BF16), v((16, 32, 128), BF16),
            v((16, 32, 128), BF16), v((4, 2, 16, 2048), BF16), v((4, 16, 2048), BF16),
            v((4, 16, 2048), BF16), v((4, 16, 2048), BF16),
            pltpu.SemaphoreType.DMA((9,)), pltpu.SemaphoreType.DMA((MESSAGES,)),
            pltpu.SemaphoreType.DMA((MESSAGES,)),
        ],
        compiler_params=pltpu.CompilerParams(
            collective_id=0, has_side_effects=True, vmem_limit_bytes=52 * 1024 * 1024),
        name="step",
    )(*(pltpu.with_memory_space_constraint(array, pltpu.HBM) for array in (
        target, source, target_gain.reshape(1, 2048), source_gain.reshape(1, 2048),
        w_query, w_key, w_value, attended, d_attended)))
    return tuple(pl.pallas_call(
        store_kernel, out_shape=outs, in_specs=[vm] * 3, out_specs=[anywhere] * 3,
        scratch_shapes=[pltpu.SemaphoreType.DMA((3,))],
        compiler_params=pltpu.CompilerParams(vmem_limit_bytes=4 * 1024 * 1024),
        name="store")(*results))


def solution(mesh):
    fine = Mesh(mesh.devices.reshape(NZ, NY, NX, NC), ("z", "y", "x", "c"))
    sp = ("z", "y")
    tp = ("x", "c")
    both = ("z", "y", "x", "c")
    placed = (P(sp, None), P(both, None), P(), P(), P(None, tp), P(), P(), P(sp, tp), P(sp, tp))
    return jax.shard_map(
        local, mesh=fine, in_specs=placed,
        out_specs=(P(sp, None), P(both, None), P(sp, tp)), check_vma=False)
```

```python
import jax
import jax.numpy as jnp
from jax import lax
from jax.experimental import pallas as pl
from jax.experimental.pallas import tpu as pltpu
from jax.sharding import Mesh
from jax.sharding import PartitionSpec as P

HD = 128
EPS = 1e-06
SCALE = HD ** (-0.5)
LOG2E = 1.4426950408889634
NZ, NY, NX, NC = 16, 4, 4, 2
MESH = pl.DeviceIdType.MESH
F32 = jnp.float32
BF16 = jnp.bfloat16
NT = (((1,), (1,)), ((), ()))
NN = (((1,), (0,)), ((), ()))
MESSAGES = 176
EARLY = 8
BASE = {0: 0, 1: 320, 3: 576, 2: 832}
SIZE = {0: 320, 1: 256, 3: 256, 2: 192}
NEAR = {0: (1, -1, 2, -2), 1: (-2, 1, -1), 3: (2, 1, -1), 2: (1, -1)}
ZORDER = (8, 7, 9, 6, 10, 5, 11, 4, 12, 3, 13, 2, 14, 1, 15, 0)


def dot(a, b, dims=NN):
    return lax.dot_general(a, b, dims, preferred_element_type=F32)


def place(k, d):
    if d == 0:
        slot = 0
    elif d == -1:
        slot = 1
    elif d == 1:
        slot = 2
    elif d == -2:
        slot = 3
    else:
        slot = 4 if k == 0 else 3
    return BASE[k] + 64 * slot


def normed(matrix, gain):
    wide = matrix.astype(F32)
    inverse = lax.rsqrt(jnp.mean(wide * wide, axis=-1, keepdims=True) + EPS)
    return (wide * inverse * gain).astype(BF16)


def normed_back(matrix, gain, cotangent):
    wide = matrix.astype(F32)
    inverse = lax.rsqrt(jnp.mean(wide * wide, axis=-1, keepdims=True) + EPS)
    scaled = cotangent * gain
    along = jnp.mean(scaled * wide, axis=-1, keepdims=True)
    return scaled * inverse - wide * (inverse * inverse * inverse * along)


def kernel(target, source, tgain, sgain, w_query, w_key, w_value, attended, d_attended,
           d_target, d_source, d_w,
           tg, sr, wq, wk, wv, tgn, sgn, att, dat, nt_t, nt_r, k_own, v_own, ks, vs, q, do, dl, own_dl,
           st, st_all, mg, lg, e_scr, pt, ut, kt, dqf, frow, dq, dq_in, q_t, do_t, q2, do2, dkv, near_in, via_in,
           far, far_in, dw, dw_in, dw1, dw2, dn, dn_pair, dn2, dn_in,
           load_sem, send_sem, recv_sem):
    z = lax.axis_index("z")
    y = lax.axis_index("y")
    x = lax.axis_index("x")
    c = lax.axis_index("c")
    xh = x // 2
    xl = lax.rem(x, 2)
    mine = y * 4 + xl * 2 + c
    tp = x * 2 + c

    def zmod(v):
        return lax.rem(v + NZ, NZ)

    def at(dz=0, dy=0, dxl=0, dc=0, dh=0):
        x2 = lax.rem(xh + dh, 2) * 2 + lax.rem(xl + dxl, 2)
        return (zmod(z + dz), lax.rem(y + dy, NY), x2, lax.rem(c + dc, 2))

    def block(dy, dxl, dc):
        return lax.rem(y + dy + NY, NY) * 4 + lax.rem(xl + dxl, 2) * 2 + lax.rem(c + dc, 2)

    def rows_of(j, n=128):
        return pl.ds(pl.multiple_of(j * n, n), n)

    count = [0]
    pending = []

    def remote(src, dst, dev):
        k = count[0]
        count[0] += 1
        cp = pltpu.make_async_remote_copy(
            src_ref=src, dst_ref=dst, send_sem=send_sem.at[k], recv_sem=recv_sem.at[k],
            device_id=dev, device_id_type=MESH)
        cp.start()
        pending.append(cp)
        return cp

    loads = []
    for k, (a, b) in enumerate(((source, sr), (sgain, sgn), (w_key, wk), (w_value, wv),
                                (target, tg), (tgain, tgn), (w_query, wq),
                                (d_attended, dat), (attended, att))):
        cp = pltpu.make_async_copy(a, b, load_sem.at[k])
        if k < 4:
            cp.start()
        loads.append(cp)

    offs = [(dy, dx, dc) for dy in (2, 1, 3, 0) for dx in (1, 0) for dc in (1, 0)][:-1]
    peers = [at(dy=a, dxl=b, dc=d) for a, b, d in offs]
    peers += [at(dz=k) for k in range(1, 16)]
    peers += [at(dz=k, dh=1) for k in (4, 8, 12)]
    peers += [at(dh=1, dxl=a, dc=b) for a in (0, 1) for b in (0, 1)]
    barrier = pltpu.get_barrier_semaphore()
    for d in peers:
        pl.semaphore_signal(barrier, inc=1, device_id=d, device_id_type=MESH)

    loads[0].wait()
    loads[1].wait()
    ns = normed(sr[...], sgn[...])
    loads[2].wait()
    loads[3].wait()
    for cp in loads[4:]:
        cp.start()
    key = dot(ns, wk[...]).astype(BF16)
    value = dot(ns, wv[...]).astype(BF16)
    for i in range(2):
        k_own[i] = key[:, i * 128:(i + 1) * 128]
        v_own[i] = value[:, i * 128:(i + 1) * 128]
    pl.semaphore_wait(barrier, len(peers))

    g1 = {}
    for which, own, full in ((0, k_own, ks), (1, v_own, vs)):
        for k, dh in ((0, 1), (2, 0), (2, 1), (1, 0), (1, 1), (3, 0), (3, 1)):
            slot = (4 - k) % 4
            g1[which, slot, dh] = remote(own.at[lax.rem(xh + dh, 2)],
                                         full.at[pl.ds(place(slot, 0) + dh * 32, 32), :],
                                         at(dz=4 * k, dh=dh))
        full[0:32, :] = own[xh]

    for k in range(4, 9):
        loads[k].wait()
    nt = normed(tg[...], tgn[...])
    q[rows_of(mine), :] = dot(nt, wq[...]).astype(BF16)
    do[rows_of(mine), :] = dat[...]
    chips = ((2, 0), (2, 1), (1, 0), (3, 0), (1, 1), (3, 1), (0, 1))
    own_q = q.at[rows_of(mine), :]
    own_do = do.at[rows_of(mine), :]
    q_send = {o: remote(own_q, own_q, at(dy=o[0], dxl=o[1])) for o in chips}
    q_pair = remote(own_q, own_q, at(dc=1))
    prod = dat[...].astype(F32) * att[...].astype(F32)
    delta = jnp.sum(jnp.transpose(prod), axis=0, keepdims=True).astype(BF16).astype(F32)
    own_dl[...] = jnp.broadcast_to(delta, (8, 128))
    dl[mine] = own_dl[...]
    do_send = {o: remote(own_do, own_do, at(dy=o[0], dxl=o[1])) for o in chips}
    do_pair = remote(own_do, own_do, at(dc=1))
    dl_send = [remote(own_dl, dl.at[mine], at(dy=a, dxl=b, dc=d)) for a, b, d in offs]
    nt_t[...] = jnp.transpose(nt)
    for i in range(16):
        nt_r[i * 128:(i + 1) * 128, :] = nt_t[rows_of(zmod(z + ZORDER[i])), :]

    near = {}

    def forward(which, k):
        full = vs if which else ks
        src = full.at[pl.ds(place(k, 0), 64), :]
        for d in NEAR[k]:
            near[which, k, d] = remote(src, full.at[pl.ds(place(k, d), 64), :], at(dz=d))

    def pass_on(sends, array):
        out = []
        for dy, dx in ((0, 1), (1, 0), (3, 0), (1, 1), (3, 1), (2, 0), (2, 1)):
            sends[dy, dx].wait_recv()
            r = array.at[rows_of(block(-dy, dx, 0)), :]
            out.append(remote(r, r, at(dc=1)))
        return out

    def arrived(which, k):
        for d in NEAR[k]:
            near[which, k, d].wait_recv()

    def relay(which, k):
        for dh in (0, 1):
            if (k, dh) != (0, 0):
                g1[which, k, dh].wait_recv()
        forward(which, k)

    def scores(k):
        base, size = BASE[k], SIZE[k]

        def pair(p):
            cols = slice(p * 256, (p + 1) * 256)
            s = dot(ks[base:base + size, :], q_t[:, cols])
            for i in range(size // 64):
                t = s[i * 64:(i + 1) * 64].reshape(8, 8, 256) * (SCALE * LOG2E)
                m = jnp.max(t, axis=0)
                e = jnp.exp2(t - m[None])
                n = base // 64 + i
                mg[n, :, cols] = m
                lg[n, :, cols] = jnp.sum(e, axis=0)
                e_scr[base + i * 64:base + (i + 1) * 64, cols] = e.reshape(64, 256)

        for p in range(8):
            pair(p)

    def finish(k, cols, p):
        base, size = BASE[k], SIZE[k]
        drow = jnp.concatenate([dl[2 * p, 0:1, :], dl[2 * p + 1, 0:1, :]], axis=1)
        g = dot(vs[base:base + size, :], do_t[:, cols]) - drow
        for i in range(size // 64):
            n = base // 64 + i
            r = slice(n * 64, (n + 1) * 64)
            w = e_scr[r, cols].reshape(8, 8, 256) * mg[n, :, cols][None]
            pt[r, cols] = w.reshape(64, 256).astype(BF16)
            u = w * g[i * 64:(i + 1) * 64].reshape(8, 8, 256)
            ut[r, cols] = u.reshape(64, 256).astype(BF16)

    relay(0, 0)
    q_fwd = pass_on(q_send, q)
    relay(0, 1)
    relay(0, 3)
    relay(1, 0)
    q_pair.wait_recv()
    for cp in q_fwd:
        cp.wait_recv()
    q_t[...] = jnp.transpose(q[...])
    arrived(0, 0)
    scores(0)
    relay(0, 2)
    do_fwd = pass_on(do_send, do)
    relay(1, 1)
    relay(1, 3)
    arrived(0, 1)
    scores(1)
    arrived(0, 3)
    scores(3)
    relay(1, 2)
    arrived(0, 2)
    scores(2)
    top8 = jnp.max(mg[...], axis=0)
    top1 = jnp.max(top8, axis=0, keepdims=True)
    tot = lg[0] * jnp.exp2(mg[0] - top1)
    for i in range(1, 16):
        tot = tot + lg[i] * jnp.exp2(mg[i] - top1)
    lse = top1 + jnp.log(jnp.sum(tot, axis=0, keepdims=True)) * LOG2E
    for j in range(16):
        st[j:j + 1, :] = lse[:, j * 128:(j + 1) * 128]
    stats = [remote(st, st_all.at[mine], at(dy=a, dxl=b, dc=d)) for a, b, d in offs]
    st_all[mine] = st[...]
    for i in range(16):
        mg[i] = jnp.exp2(mg[i] - lse)
    kt[...] = jnp.transpose(ks[...])
    do_pair.wait_recv()
    for cp in do_fwd + dl_send:
        cp.wait_recv()
    do_t[...] = jnp.transpose(do[...])
    for k in (0, 1, 3):
        arrived(1, k)
        for p in range(8):
            finish(k, slice(p * 256, (p + 1) * 256), p)
    arrived(1, 2)

    def grads(dy, dx):
        p = lax.rem(y + dy, NY) * 2 + lax.rem(xl + dx, 2)
        cols = rows_of(p, 256)
        finish(2, cols, p)
        return cols, dot(kt[...], ut[:, cols]) * SCALE

    order = ((2, 1), (2, 0), (1, 1), (3, 1), (1, 0), (3, 0), (0, 1), (0, 0))
    dq_send = []

    def dq_out(cols, value, dy, dx):
        dq[cols, :] = jnp.transpose(value * frow[0:1, cols]).astype(BF16)
        for dc in (1, 0):
            if (dy, dx, dc) != (0, 0, 0):
                dq_send.append(remote(dq.at[rows_of(block(dy, dx, dc)), :], dq_in.at[mine],
                                      at(dy=dy, dxl=dx, dc=dc)))

    held = []
    for dy, dx in order[:EARLY]:
        cols, value = grads(dy, dx)
        dqf[:, cols] = value
        held.append((cols, dy, dx))
    for cp in stats:
        cp.wait_recv()
    top = jnp.max(st_all[...], axis=0)
    total = jnp.zeros((16, 128), F32)
    for j in range(16):
        total = total + jnp.exp2(st_all[j] - top)
    factor = jnp.exp2(st[...] - (top + jnp.log(total) * LOG2E))
    factor_t = jnp.transpose(jnp.concatenate([factor, jnp.zeros((112, 128), F32)], axis=0))
    for j in range(16):
        frow[0:1, j * 128:(j + 1) * 128] = factor[j:j + 1, :]
    for cols, dy, dx in held:
        dq_out(cols, dqf[:, cols], dy, dx)
    for dy, dx in order[EARLY:]:
        cols, value = grads(dy, dx)
        dq_out(cols, value, dy, dx)
    dq_in[mine] = dq[rows_of(mine), :]
    for j in range(16):
        r = slice(j * 128, (j + 1) * 128)
        f = factor_t[:, j:j + 1]
        q2[r, :] = (q[r, :].astype(F32) * f).astype(BF16)
        do2[r, :] = (do[r, :].astype(F32) * f).astype(BF16)
    back = {}
    index = 0
    for k in (2, 1, 3, 0):
        r = slice(BASE[k], BASE[k] + SIZE[k])
        dk = dot(ut[r, :], q2[...]) * SCALE
        dv = dot(pt[r, :], do2[...])
        dkv[r, :] = jnp.concatenate([dk, dv], axis=1).astype(BF16)
        for d in NEAR[k]:
            back[k, d] = (remote(dkv.at[pl.ds(place(k, d), 64), :], near_in.at[index], at(dz=-d)),
                          index)
            index += 1

    for cp in dq_send:
        cp.wait_recv()
    acc = dq_in[0].astype(F32)
    for j in range(1, 16):
        acc = acc + dq_in[j].astype(F32)
    dqb = acc.astype(BF16)
    w_all = dot(nt_r[...], dqb).astype(BF16)
    dn_all = dot(dqb, wq[...], NT).astype(BF16)
    dw[...] = w_all.reshape(16, 4, 32, 128)
    w_send = ([], [], [], [])
    for part in range(4):
        for d in (2, 1, 3):
            some = pl.ds(4 * part, 4)
            w_send[part].append(remote(dw.at[some, lax.rem(y + d, NY)], dw_in.at[some, y],
                                       at(dy=d)))
        if part == 1:
            dn[...] = dn_all.reshape(4, 2, 16, 2048)
            pair_send = remote(dn.at[:, lax.rem(c + 1, 2)], dn_pair, at(dc=1))
    dw_in[:, y] = dw[:, y]

    pair_send.wait_recv()
    dn2[...] = (dn[:, c].astype(F32) + dn_pair[...].astype(F32)).astype(BF16)
    n_send = []
    for a, b in ((1, 0), (1, 1), (0, 1)):
        dev = at(dh=a, dxl=b)
        n_send.append(remote(dn2.at[dev[2]], dn_in.at[x], dev))
    dn_in[x] = dn2[x]

    f_send = []
    via = {}

    def far_out(k, dh):
        f_send.append(remote(far.at[pl.ds(k * 64 + dh * 32, 32), :], far_in.at[dh, k],
                             at(dz=4 * k, dh=dh)))

    for k in (2, 1, 3, 0):
        total_k = dkv[place(k, 0):place(k, 0) + 64, :].astype(F32)
        for d in NEAR[k]:
            cp, i = back[k, d]
            cp.wait_recv()
            total_k = total_k + near_in[i].astype(F32)
        far[k * 64:(k + 1) * 64, :] = total_k.astype(BF16)
        for dh in (0, 1):
            if k == 2:
                via[dh] = remote(far.at[pl.ds(k * 64 + dh * 32, 32), :], via_in.at[dh],
                                 at(dz=-4 if dh else 4))
            elif (k, dh) not in ((0, 0), (1, 0), (3, 1)):
                far_out(k, dh)
    far_in[0, 0] = far[0:32, :]

    z_send = []

    def z_part(part):
        for cp in w_send[part]:
            cp.wait_recv()
        half = slice(4 * part, 4 * part + 4)
        wsum = dw_in[half, 0].astype(F32)
        for j in range(1, 4):
            wsum = wsum + dw_in[half, j].astype(F32)
        dw1[half] = wsum.astype(BF16)
        for i in range(4 * part, 4 * part + 4):
            if ZORDER[i]:
                z_send.append(remote(dw1.at[i], dw2.at[i], at(dz=ZORDER[i])))

    z_part(0)
    z_part(1)
    for k, dh in ((1, 0), (3, 1)):
        via[dh].wait_recv()
        r = slice(k * 64 + dh * 32, k * 64 + dh * 32 + 32)
        far[r, :] = (far[r, :].astype(F32) + via_in[dh].astype(F32)).astype(BF16)
        far_out(k, dh)
    z_part(2)
    z_part(3)
    dw2[15] = dw1[15]

    for cp in n_send:
        cp.wait_recv()
    nsum = dn_in[0].astype(F32)
    for j in range(1, 4):
        nsum = nsum + dn_in[j].astype(F32)
    own_rows = rows_of(tp, 16)
    d_target[own_rows, :] = normed_back(tg[own_rows, :], tgn[...], nsum).astype(BF16)
    own_t = d_target.at[own_rows, :]
    t_send = {}
    for a, b in ((1, 0), (1, 1), (0, 1)):
        t_send[a, b] = remote(own_t, own_t, at(dh=a, dxl=b))
    t_pair = remote(own_t, own_t, at(dc=1))
    t_fwd = []
    for a, b in ((0, 1), (1, 0), (1, 1)):
        t_send[a, b].wait_recv()
        x2 = lax.rem(xh + a, 2) * 2 + lax.rem(xl + b, 2)
        r = d_target.at[rows_of(x2 * 2 + c, 16), :]
        t_fwd.append(remote(r, r, at(dc=1)))

    for cp in f_send:
        cp.wait_recv()
    fs = []
    for dh in range(2):
        v = far_in[dh, 0].astype(F32)
        for k in (1, 3):
            v = v + far_in[dh, k].astype(F32)
        fs.append(v)
    low = jnp.where(xh == 0, fs[0], fs[1]).astype(BF16)
    high = jnp.where(xh == 0, fs[1], fs[0]).astype(BF16)
    dkey = jnp.concatenate([low[:, :128], high[:, :128]], axis=1)
    dval = jnp.concatenate([low[:, 128:], high[:, 128:]], axis=1)
    dns = dot(dkey, wk[...], NT) + dot(dval, wv[...], NT)
    d_source[...] = normed_back(sr[...], sgn[...], dns)

    for cp in pending:
        cp.wait_send()
    for cp in z_send:
        cp.wait_recv()
    zsum = dw2[0].astype(F32)
    for j in range(1, 16):
        zsum = zsum + dw2[j].astype(F32)
    d_w[...] = zsum
    t_pair.wait_recv()
    for cp in t_fwd:
        cp.wait_recv()
    assert count[0] <= MESSAGES


def store_kernel(a, b, w, a_out, b_out, w_out, sem):
    copies = [pltpu.make_async_copy(s, d, sem.at[k])
              for k, (s, d) in enumerate(((a, a_out), (b, b_out), (w, w_out)))]
    for cp in copies:
        cp.start()
    for cp in copies:
        cp.wait()


def local(target, source, target_gain, source_gain, w_query, w_key, w_value, attended, d_attended):
    vm = pl.BlockSpec(memory_space=pltpu.VMEM)
    anywhere = pl.BlockSpec(memory_space=pltpu.HBM)
    v = pltpu.VMEM
    outs = [jax.ShapeDtypeStruct((128, 2048), BF16), jax.ShapeDtypeStruct((32, 2048), F32),
            jax.ShapeDtypeStruct((32, 128), F32)]
    results = pl.pallas_call(
        kernel,
        out_shape=outs,
        in_specs=[anywhere] * 9,
        out_specs=[vm, vm, vm],
        scratch_shapes=[
            v((128, 2048), BF16), v((32, 2048), BF16), v((2048, 128), BF16),
            v((2048, 256), BF16), v((2048, 256), BF16), v((1, 2048), F32), v((1, 2048), F32),
            v((128, 128), BF16), v((128, 128), BF16), v((2048, 128), BF16), v((2048, 128), BF16),
            v((2, 32, 128), BF16), v((2, 32, 128), BF16), v((1024, 128), BF16),
            v((1024, 128), BF16), v((2048, 128), BF16), v((2048, 128), BF16),
            v((16, 8, 128), F32), v((8, 128), F32),
            v((16, 128), F32), v((16, 16, 128), F32), v((16, 8, 2048), F32), v((16, 8, 2048), F32),
            v((1024, 2048), F32),
            v((1024, 2048), BF16), v((1024, 2048), BF16), v((128, 1024), BF16),
            v((128, 2048), F32), v((8, 2048), F32), v((2048, 128), BF16),
            v((16, 128, 128), BF16),
            v((128, 2048), BF16), v((128, 2048), BF16),
            v((2048, 128), BF16), v((2048, 128), BF16), v((1024, 256), BF16),
            v((12, 64, 256), BF16), v((2, 32, 256), BF16), v((256, 256), BF16), v((2, 4, 32, 256), BF16),
            v((16, 4, 32, 128), BF16), v((16, 4, 32, 128), BF16), v((16, 32, 128), BF16),
            v((16, 32, 128), BF16), v((4, 2, 16, 2048), BF16), v((4, 16, 2048), BF16),
            v((4, 16, 2048), BF16), v((4, 16, 2048), BF16),
            pltpu.SemaphoreType.DMA((9,)), pltpu.SemaphoreType.DMA((MESSAGES,)),
            pltpu.SemaphoreType.DMA((MESSAGES,)),
        ],
        compiler_params=pltpu.CompilerParams(
            collective_id=0, has_side_effects=True, vmem_limit_bytes=52 * 1024 * 1024),
        name="step",
    )(*(pltpu.with_memory_space_constraint(array, pltpu.HBM) for array in (
        target, source, target_gain.reshape(1, 2048), source_gain.reshape(1, 2048),
        w_query, w_key, w_value, attended, d_attended)))
    return tuple(pl.pallas_call(
        store_kernel, out_shape=outs, in_specs=[vm] * 3, out_specs=[anywhere] * 3,
        scratch_shapes=[pltpu.SemaphoreType.DMA((3,))],
        compiler_params=pltpu.CompilerParams(vmem_limit_bytes=4 * 1024 * 1024),
        name="store")(*results))


def solution(mesh):
    fine = Mesh(mesh.devices.reshape(NZ, NY, NX, NC), ("z", "y", "x", "c"))
    sp = ("z", "y")
    tp = ("x", "c")
    both = ("z", "y", "x", "c")
    placed = (P(sp, None), P(both, None), P(), P(), P(None, tp), P(), P(), P(sp, tp), P(sp, tp))
    return jax.shard_map(
        local, mesh=fine, in_specs=placed,
        out_specs=(P(sp, None), P(both, None), P(sp, tp)), check_vma=False)
```

```python
import jax
import jax.numpy as jnp
from jax import lax
from jax.experimental import pallas as pl
from jax.experimental.pallas import tpu as pltpu
from jax.sharding import Mesh
from jax.sharding import PartitionSpec as P

HD = 128
EPS = 1e-06
SCALE = HD ** (-0.5)
LOG2E = 1.4426950408889634
NZ, NY, NX, NC = 16, 4, 4, 2
MESH = pl.DeviceIdType.MESH
F32 = jnp.float32
BF16 = jnp.bfloat16
NT = (((1,), (1,)), ((), ()))
NN = (((1,), (0,)), ((), ()))
MESSAGES = 176
EARLY = 8
BASE = {0: 0, 1: 320, 3: 576, 2: 832}
SIZE = {0: 320, 1: 256, 3: 256, 2: 192}
NEAR = {0: (1, -1, 2, -2), 1: (-2, 1, -1), 3: (2, 1, -1), 2: (1, -1)}
ZORDER = (8, 7, 9, 6, 10, 5, 11, 4, 12, 3, 13, 2, 14, 1, 15, 0)


def dot(a, b, dims=NN):
    return lax.dot_general(a, b, dims, preferred_element_type=F32)


def place(k, d):
    if d == 0:
        slot = 0
    elif d == -1:
        slot = 1
    elif d == 1:
        slot = 2
    elif d == -2:
        slot = 3
    else:
        slot = 4 if k == 0 else 3
    return BASE[k] + 64 * slot


def normed(matrix, gain):
    wide = matrix.astype(F32)
    inverse = lax.rsqrt(jnp.mean(wide * wide, axis=-1, keepdims=True) + EPS)
    return (wide * inverse * gain).astype(BF16)


def normed_back(matrix, gain, cotangent):
    wide = matrix.astype(F32)
    inverse = lax.rsqrt(jnp.mean(wide * wide, axis=-1, keepdims=True) + EPS)
    scaled = cotangent * gain
    along = jnp.mean(scaled * wide, axis=-1, keepdims=True)
    return scaled * inverse - wide * (inverse * inverse * inverse * along)


def kernel(target, source, tgain, sgain, w_query, w_key, w_value, attended, d_attended,
           d_target, d_source, d_w,
           tg, sr, wq, wk, wv, tgn, sgn, att, dat, nt_t, nt_r, k_own, v_own, ks, vs, q, do, dl, own_dl,
           st, st_all, mg, lg, e_scr, pt, ut, kt, dqf, frow, dq, dq_in, q_t, do_t, q2, do2, dkv, near_in, via_in,
           far, far_in, dw, dw_in, dw1, dw2, dn, dn_pair, dn2, dn_in,
           load_sem, send_sem, recv_sem):
    z = lax.axis_index("z")
    y = lax.axis_index("y")
    x = lax.axis_index("x")
    c = lax.axis_index("c")
    xh = x // 2
    xl = lax.rem(x, 2)
    mine = y * 4 + xl * 2 + c
    tp = x * 2 + c

    def zmod(v):
        return lax.rem(v + NZ, NZ)

    def at(dz=0, dy=0, dxl=0, dc=0, dh=0):
        x2 = lax.rem(xh + dh, 2) * 2 + lax.rem(xl + dxl, 2)
        return (zmod(z + dz), lax.rem(y + dy, NY), x2, lax.rem(c + dc, 2))

    def block(dy, dxl, dc):
        return lax.rem(y + dy + NY, NY) * 4 + lax.rem(xl + dxl, 2) * 2 + lax.rem(c + dc, 2)

    def rows_of(j, n=128):
        return pl.ds(pl.multiple_of(j * n, n), n)

    count = [0]
    pending = []

    def remote(src, dst, dev):
        k = count[0]
        count[0] += 1
        cp = pltpu.make_async_remote_copy(
            src_ref=src, dst_ref=dst, send_sem=send_sem.at[k], recv_sem=recv_sem.at[k],
            device_id=dev, device_id_type=MESH)
        cp.start()
        pending.append(cp)
        return cp

    loads = []
    for k, (a, b) in enumerate(((source, sr), (sgain, sgn), (w_key, wk), (w_value, wv),
                                (target, tg), (tgain, tgn), (w_query, wq),
                                (d_attended, dat), (attended, att))):
        cp = pltpu.make_async_copy(a, b, load_sem.at[k])
        if k < 4:
            cp.start()
        loads.append(cp)

    offs = [(dy, dx, dc) for dy in (2, 1, 3, 0) for dx in (1, 0) for dc in (1, 0)][:-1]
    peers = [at(dy=a, dxl=b, dc=d) for a, b, d in offs]
    peers += [at(dz=k) for k in range(1, 16)]
    peers += [at(dz=k, dh=1) for k in (4, 8, 12)]
    peers += [at(dh=1, dxl=a, dc=b) for a in (0, 1) for b in (0, 1)]
    barrier = pltpu.get_barrier_semaphore()
    for d in peers:
        pl.semaphore_signal(barrier, inc=1, device_id=d, device_id_type=MESH)

    loads[0].wait()
    loads[1].wait()
    ns = normed(sr[...], sgn[...])
    loads[2].wait()
    loads[3].wait()
    for cp in loads[4:]:
        cp.start()
    key = dot(ns, wk[...]).astype(BF16)
    value = dot(ns, wv[...]).astype(BF16)
    for i in range(2):
        k_own[i] = key[:, i * 128:(i + 1) * 128]
        v_own[i] = value[:, i * 128:(i + 1) * 128]
    pl.semaphore_wait(barrier, len(peers))

    g1 = {}
    for which, own, full in ((0, k_own, ks), (1, v_own, vs)):
        for k, dh in ((0, 1), (2, 0), (2, 1), (1, 0), (1, 1), (3, 0), (3, 1)):
            slot = (4 - k) % 4
            g1[which, slot, dh] = remote(own.at[lax.rem(xh + dh, 2)],
                                         full.at[pl.ds(place(slot, 0) + dh * 32, 32), :],
                                         at(dz=4 * k, dh=dh))
        full[0:32, :] = own[xh]

    for k in range(4, 9):
        loads[k].wait()
    nt = normed(tg[...], tgn[...])
    q[rows_of(mine), :] = dot(nt, wq[...]).astype(BF16)
    do[rows_of(mine), :] = dat[...]
    chips = ((2, 0), (2, 1), (1, 0), (3, 0), (1, 1), (3, 1), (0, 1))
    own_q = q.at[rows_of(mine), :]
    own_do = do.at[rows_of(mine), :]
    q_send = {o: remote(own_q, own_q, at(dy=o[0], dxl=o[1])) for o in chips}
    q_pair = remote(own_q, own_q, at(dc=1))
    prod = dat[...].astype(F32) * att[...].astype(F32)
    delta = jnp.sum(jnp.transpose(prod), axis=0, keepdims=True).astype(BF16).astype(F32)
    own_dl[...] = jnp.broadcast_to(delta, (8, 128))
    dl[mine] = own_dl[...]
    do_send = {o: remote(own_do, own_do, at(dy=o[0], dxl=o[1])) for o in chips}
    do_pair = remote(own_do, own_do, at(dc=1))
    dl_send = [remote(own_dl, dl.at[mine], at(dy=a, dxl=b, dc=d)) for a, b, d in offs]
    nt_t[...] = jnp.transpose(nt)
    for i in range(16):
        nt_r[i * 128:(i + 1) * 128, :] = nt_t[rows_of(zmod(z + ZORDER[i])), :]

    near = {}

    def forward(which, k):
        full = vs if which else ks
        src = full.at[pl.ds(place(k, 0), 64), :]
        for d in NEAR[k]:
            near[which, k, d] = remote(src, full.at[pl.ds(place(k, d), 64), :], at(dz=d))

    def pass_on(sends, array):
        out = []
        for dy, dx in ((0, 1), (1, 0), (3, 0), (1, 1), (3, 1), (2, 0), (2, 1)):
            sends[dy, dx].wait_recv()
            r = array.at[rows_of(block(-dy, dx, 0)), :]
            out.append(remote(r, r, at(dc=1)))
        return out

    def arrived(which, k):
        for d in NEAR[k]:
            near[which, k, d].wait_recv()

    def relay(which, k):
        for dh in (0, 1):
            if (k, dh) != (0, 0):
                g1[which, k, dh].wait_recv()
        forward(which, k)

    def scores(k):
        base, size = BASE[k], SIZE[k]

        def pair(p):
            cols = slice(p * 256, (p + 1) * 256)
            s = dot(ks[base:base + size, :], q_t[:, cols])
            for i in range(size // 64):
                t = s[i * 64:(i + 1) * 64].reshape(8, 8, 256) * (SCALE * LOG2E)
                m = jnp.max(t, axis=0)
                e = jnp.exp2(t - m[None])
                n = base // 64 + i
                mg[n, :, cols] = m
                lg[n, :, cols] = jnp.sum(e, axis=0)
                e_scr[base + i * 64:base + (i + 1) * 64, cols] = e.reshape(64, 256)

        for p in range(8):
            pair(p)

    def finish(k, cols, p):
        base, size = BASE[k], SIZE[k]
        drow = jnp.concatenate([dl[2 * p, 0:1, :], dl[2 * p + 1, 0:1, :]], axis=1)
        g = dot(vs[base:base + size, :], do_t[:, cols]) - drow
        for i in range(size // 64):
            n = base // 64 + i
            r = slice(n * 64, (n + 1) * 64)
            w = e_scr[r, cols].reshape(8, 8, 256) * mg[n, :, cols][None]
            pt[r, cols] = w.reshape(64, 256).astype(BF16)
            u = w * g[i * 64:(i + 1) * 64].reshape(8, 8, 256)
            ut[r, cols] = u.reshape(64, 256).astype(BF16)

    relay(0, 0)
    q_fwd = pass_on(q_send, q)
    relay(0, 1)
    relay(0, 3)
    relay(1, 0)
    q_pair.wait_recv()
    for cp in q_fwd:
        cp.wait_recv()
    q_t[...] = jnp.transpose(q[...])
    arrived(0, 0)
    scores(0)
    relay(0, 2)
    do_fwd = pass_on(do_send, do)
    relay(1, 1)
    relay(1, 3)
    arrived(0, 1)
    scores(1)
    arrived(0, 3)
    scores(3)
    relay(1, 2)
    arrived(0, 2)
    scores(2)
    top8 = jnp.max(mg[...], axis=0)
    top1 = jnp.max(top8, axis=0, keepdims=True)
    tot = lg[0] * jnp.exp2(mg[0] - top1)
    for i in range(1, 16):
        tot = tot + lg[i] * jnp.exp2(mg[i] - top1)
    lse = top1 + jnp.log(jnp.sum(tot, axis=0, keepdims=True)) * LOG2E
    for j in range(16):
        st[j:j + 1, :] = lse[:, j * 128:(j + 1) * 128]
    stats = [remote(st, st_all.at[mine], at(dy=a, dxl=b, dc=d)) for a, b, d in offs]
    st_all[mine] = st[...]
    for i in range(16):
        mg[i] = jnp.exp2(mg[i] - lse)
    kt[...] = jnp.transpose(ks[...])
    do_pair.wait_recv()
    for cp in do_fwd + dl_send:
        cp.wait_recv()
    do_t[...] = jnp.transpose(do[...])
    for k in (0, 1, 3):
        arrived(1, k)
        for p in range(8):
            finish(k, slice(p * 256, (p + 1) * 256), p)
    arrived(1, 2)

    def grads(dy, dx):
        p = lax.rem(y + dy, NY) * 2 + lax.rem(xl + dx, 2)
        cols = rows_of(p, 256)
        finish(2, cols, p)
        return cols, dot(kt[...], ut[:, cols]) * SCALE

    order = ((2, 1), (2, 0), (1, 1), (3, 1), (1, 0), (3, 0), (0, 1), (0, 0))
    dq_send = []

    def dq_out(cols, value, dy, dx):
        dq[cols, :] = jnp.transpose(value * frow[0:1, cols]).astype(BF16)
        for dc in (1, 0):
            if (dy, dx, dc) != (0, 0, 0):
                dq_send.append(remote(dq.at[rows_of(block(dy, dx, dc)), :], dq_in.at[mine],
                                      at(dy=dy, dxl=dx, dc=dc)))

    held = []
    for dy, dx in order[:EARLY]:
        cols, value = grads(dy, dx)
        dqf[:, cols] = value
        held.append((cols, dy, dx))
    for cp in stats:
        cp.wait_recv()
    top = jnp.max(st_all[...], axis=0)
    total = jnp.zeros((16, 128), F32)
    for j in range(16):
        total = total + jnp.exp2(st_all[j] - top)
    factor = jnp.exp2(st[...] - (top + jnp.log(total) * LOG2E))
    factor_t = jnp.transpose(jnp.concatenate([factor, jnp.zeros((112, 128), F32)], axis=0))
    for j in range(16):
        frow[0:1, j * 128:(j + 1) * 128] = factor[j:j + 1, :]
    for cols, dy, dx in held:
        dq_out(cols, dqf[:, cols], dy, dx)
    for dy, dx in order[EARLY:]:
        cols, value = grads(dy, dx)
        dq_out(cols, value, dy, dx)
    dq_in[mine] = dq[rows_of(mine), :]
    for j in range(16):
        r = slice(j * 128, (j + 1) * 128)
        f = factor_t[:, j:j + 1]
        q2[r, :] = (q[r, :].astype(F32) * f).astype(BF16)
        do2[r, :] = (do[r, :].astype(F32) * f).astype(BF16)
    back = {}
    index = 0
    for k in (2, 1, 3, 0):
        r = slice(BASE[k], BASE[k] + SIZE[k])
        dk = dot(ut[r, :], q2[...]) * SCALE
        dv = dot(pt[r, :], do2[...])
        dkv[r, :] = jnp.concatenate([dk, dv], axis=1).astype(BF16)
        for d in NEAR[k]:
            back[k, d] = (remote(dkv.at[pl.ds(place(k, d), 64), :], near_in.at[index], at(dz=-d)),
                          index)
            index += 1

    for cp in dq_send:
        cp.wait_recv()
    acc = dq_in[0].astype(F32)
    for j in range(1, 16):
        acc = acc + dq_in[j].astype(F32)
    dqb = acc.astype(BF16)
    w_all = dot(nt_r[...], dqb).astype(BF16)
    dn_all = dot(dqb, wq[...], NT).astype(BF16)
    dw[...] = w_all.reshape(16, 4, 32, 128)
    w_send = ([], [], [], [])
    for part in range(4):
        for d in (2, 1, 3):
            some = pl.ds(4 * part, 4)
            w_send[part].append(remote(dw.at[some, lax.rem(y + d, NY)], dw_in.at[some, y],
                                       at(dy=d)))
        if part == 1:
            dn[...] = dn_all.reshape(4, 2, 16, 2048)
            pair_send = remote(dn.at[:, lax.rem(c + 1, 2)], dn_pair, at(dc=1))
    dw_in[:, y] = dw[:, y]

    pair_send.wait_recv()
    dn2[...] = (dn[:, c].astype(F32) + dn_pair[...].astype(F32)).astype(BF16)
    n_send = []
    for a, b in ((1, 0), (1, 1), (0, 1)):
        dev = at(dh=a, dxl=b)
        n_send.append(remote(dn2.at[dev[2]], dn_in.at[x], dev))
    dn_in[x] = dn2[x]

    f_send = []
    via = {}

    def far_out(k, dh):
        f_send.append(remote(far.at[pl.ds(k * 64 + dh * 32, 32), :], far_in.at[dh, k],
                             at(dz=4 * k, dh=dh)))

    for k in (2, 1, 3, 0):
        total_k = dkv[place(k, 0):place(k, 0) + 64, :].astype(F32)
        for d in NEAR[k]:
            cp, i = back[k, d]
            cp.wait_recv()
            total_k = total_k + near_in[i].astype(F32)
        far[k * 64:(k + 1) * 64, :] = total_k.astype(BF16)
        for dh in (0, 1):
            if k == 2:
                via[dh] = remote(far.at[pl.ds(k * 64 + dh * 32, 32), :], via_in.at[dh],
                                 at(dz=-4 if dh else 4))
            elif (k, dh) not in ((0, 0), (1, 0), (3, 1)):
                far_out(k, dh)
    far_in[0, 0] = far[0:32, :]

    z_send = []

    def z_part(part):
        for cp in w_send[part]:
            cp.wait_recv()
        half = slice(4 * part, 4 * part + 4)
        wsum = dw_in[half, 0].astype(F32)
        for j in range(1, 4):
            wsum = wsum + dw_in[half, j].astype(F32)
        dw1[half] = wsum.astype(BF16)
        for i in range(4 * part, 4 * part + 4):
            if ZORDER[i]:
                z_send.append(remote(dw1.at[i], dw2.at[i], at(dz=ZORDER[i])))

    z_part(0)
    z_part(1)
    z_part(2)
    z_part(3)
    for k, dh in ((1, 0), (3, 1)):
        via[dh].wait_recv()
        r = slice(k * 64 + dh * 32, k * 64 + dh * 32 + 32)
        far[r, :] = (far[r, :].astype(F32) + via_in[dh].astype(F32)).astype(BF16)
        far_out(k, dh)
    dw2[15] = dw1[15]

    for cp in n_send:
        cp.wait_recv()
    nsum = dn_in[0].astype(F32)
    for j in range(1, 4):
        nsum = nsum + dn_in[j].astype(F32)
    own_rows = rows_of(tp, 16)
    d_target[own_rows, :] = normed_back(tg[own_rows, :], tgn[...], nsum).astype(BF16)
    own_t = d_target.at[own_rows, :]
    t_send = {}
    for a, b in ((1, 0), (1, 1), (0, 1)):
        t_send[a, b] = remote(own_t, own_t, at(dh=a, dxl=b))
    t_pair = remote(own_t, own_t, at(dc=1))
    t_fwd = []
    for a, b in ((0, 1), (1, 0), (1, 1)):
        t_send[a, b].wait_recv()
        x2 = lax.rem(xh + a, 2) * 2 + lax.rem(xl + b, 2)
        r = d_target.at[rows_of(x2 * 2 + c, 16), :]
        t_fwd.append(remote(r, r, at(dc=1)))

    for cp in f_send:
        cp.wait_recv()
    fs = []
    for dh in range(2):
        v = far_in[dh, 0].astype(F32)
        for k in (1, 3):
            v = v + far_in[dh, k].astype(F32)
        fs.append(v)
    low = jnp.where(xh == 0, fs[0], fs[1]).astype(BF16)
    high = jnp.where(xh == 0, fs[1], fs[0]).astype(BF16)
    dkey = jnp.concatenate([low[:, :128], high[:, :128]], axis=1)
    dval = jnp.concatenate([low[:, 128:], high[:, 128:]], axis=1)
    dns = dot(dkey, wk[...], NT) + dot(dval, wv[...], NT)
    d_source[...] = normed_back(sr[...], sgn[...], dns)

    for cp in pending:
        cp.wait_send()
    for cp in z_send:
        cp.wait_recv()
    zsum = dw2[0].astype(F32)
    for j in range(1, 16):
        zsum = zsum + dw2[j].astype(F32)
    d_w[...] = zsum
    t_pair.wait_recv()
    for cp in t_fwd:
        cp.wait_recv()
    assert count[0] <= MESSAGES


def store_kernel(a, b, w, a_out, b_out, w_out, sem):
    copies = [pltpu.make_async_copy(s, d, sem.at[k])
              for k, (s, d) in enumerate(((a, a_out), (b, b_out), (w, w_out)))]
    for cp in copies:
        cp.start()
    for cp in copies:
        cp.wait()


def local(target, source, target_gain, source_gain, w_query, w_key, w_value, attended, d_attended):
    vm = pl.BlockSpec(memory_space=pltpu.VMEM)
    anywhere = pl.BlockSpec(memory_space=pltpu.HBM)
    v = pltpu.VMEM
    outs = [jax.ShapeDtypeStruct((128, 2048), BF16), jax.ShapeDtypeStruct((32, 2048), F32),
            jax.ShapeDtypeStruct((32, 128), F32)]
    results = pl.pallas_call(
        kernel,
        out_shape=outs,
        in_specs=[anywhere] * 9,
        out_specs=[vm, vm, vm],
        scratch_shapes=[
            v((128, 2048), BF16), v((32, 2048), BF16), v((2048, 128), BF16),
            v((2048, 256), BF16), v((2048, 256), BF16), v((1, 2048), F32), v((1, 2048), F32),
            v((128, 128), BF16), v((128, 128), BF16), v((2048, 128), BF16), v((2048, 128), BF16),
            v((2, 32, 128), BF16), v((2, 32, 128), BF16), v((1024, 128), BF16),
            v((1024, 128), BF16), v((2048, 128), BF16), v((2048, 128), BF16),
            v((16, 8, 128), F32), v((8, 128), F32),
            v((16, 128), F32), v((16, 16, 128), F32), v((16, 8, 2048), F32), v((16, 8, 2048), F32),
            v((1024, 2048), F32),
            v((1024, 2048), BF16), v((1024, 2048), BF16), v((128, 1024), BF16),
            v((128, 2048), F32), v((8, 2048), F32), v((2048, 128), BF16),
            v((16, 128, 128), BF16),
            v((128, 2048), BF16), v((128, 2048), BF16),
            v((2048, 128), BF16), v((2048, 128), BF16), v((1024, 256), BF16),
            v((12, 64, 256), BF16), v((2, 32, 256), BF16), v((256, 256), BF16), v((2, 4, 32, 256), BF16),
            v((16, 4, 32, 128), BF16), v((16, 4, 32, 128), BF16), v((16, 32, 128), BF16),
            v((16, 32, 128), BF16), v((4, 2, 16, 2048), BF16), v((4, 16, 2048), BF16),
            v((4, 16, 2048), BF16), v((4, 16, 2048), BF16),
            pltpu.SemaphoreType.DMA((9,)), pltpu.SemaphoreType.DMA((MESSAGES,)),
            pltpu.SemaphoreType.DMA((MESSAGES,)),
        ],
        compiler_params=pltpu.CompilerParams(
            collective_id=0, has_side_effects=True, vmem_limit_bytes=52 * 1024 * 1024),
        name="step",
    )(*(pltpu.with_memory_space_constraint(array, pltpu.HBM) for array in (
        target, source, target_gain.reshape(1, 2048), source_gain.reshape(1, 2048),
        w_query, w_key, w_value, attended, d_attended)))
    return tuple(pl.pallas_call(
        store_kernel, out_shape=outs, in_specs=[vm] * 3, out_specs=[anywhere] * 3,
        scratch_shapes=[pltpu.SemaphoreType.DMA((3,))],
        compiler_params=pltpu.CompilerParams(vmem_limit_bytes=4 * 1024 * 1024),
        name="store")(*results))


def solution(mesh):
    fine = Mesh(mesh.devices.reshape(NZ, NY, NX, NC), ("z", "y", "x", "c"))
    sp = ("z", "y")
    tp = ("x", "c")
    both = ("z", "y", "x", "c")
    placed = (P(sp, None), P(both, None), P(), P(), P(None, tp), P(), P(), P(sp, tp), P(sp, tp))
    return jax.shard_map(
        local, mesh=fine, in_specs=placed,
        out_specs=(P(sp, None), P(both, None), P(sp, tp)), check_vma=False)
```
